256 devices in a mesh: ep: 16 (over y, x), tp: 16 (over z, core).
Axes of the slice: x: 4, y: 4, z: 8, core: 2. Of those that a mesh axis runs over, the one named last changes fastest.
Arguments:
- hidden_in: bfloat16 [256, 4096], P('ep'), may hold values from -6 to 6
- attn_gain: float32 [4096], replicated, may hold values from 0.1 to 1.9
- query_weight: bfloat16 [4096, 4096], P('ep', 'tp'), may hold values from -0.09375 to 0.09375
- key_weight: bfloat16 [4096, 2048], P('ep', 'tp'), may hold values from -0.09375 to 0.09375
- value_weight: bfloat16 [4096, 2048], P('ep', 'tp'), may hold values from -0.09375 to 0.09375
- query_gain: float32 [128], replicated, may hold values from 0.1 to 1.9
- key_gain: float32 [128], replicated, may hold values from 0.1 to 1.9
- head_offset: float32 [32], P('tp'), may hold values from -7 to -2
- key_cache: bfloat16 [256, 1024, 2048], P('ep', None, 'tp'), may hold values from -6 to 6
- value_cache: bfloat16 [256, 1024, 2048], P('ep', None, 'tp'), may hold values from -6 to 6
- lengths: int32 [256], P('ep'), may hold values from 1 to 1024
- out_weight: bfloat16 [4096, 4096], P('tp', 'ep'), may hold values from -0.375 to 0.375
- expert_gain: float32 [4096], replicated, may hold values from 0.1 to 1.9
- routes: int32 [256, 2], P('ep'), may hold values from 0 to 15, all different within a row; in each aligned block of 16 rows (0 to 15, 16 to 31, ...) at most 4 rows name the same one
- route_weights: float32 [256, 2], P('ep'), may hold values from 0.1 to 1
- gate_weight: bfloat16 [16, 4096, 2048], P('ep', None, 'tp'), may hold values from -0.09375 to 0.09375
- up_weight: bfloat16 [16, 4096, 2048], P('ep', None, 'tp'), may hold values from -0.09375 to 0.09375
- down_weight: bfloat16 [16, 2048, 4096], P('ep', 'tp'), may hold values from -0.125 to 0.125
Outputs:
- layer_out: bfloat16 [256, 4096], P('ep', 'tp')
- fresh_keys: bfloat16 [256, 2048], P('ep', 'tp')
- fresh_values: bfloat16 [256, 2048], P('ep', 'tp')
The draws below stay inside these ranges and needn't reach their ends.
Inputs may be any that keep to these rules, and one draw needn't show every extreme that they name: `routes`: each row names 2 different experts. Among the rows of one index of ep (16 rows) no expert is named more than 4 times, a bound that some block reaches.
All inputs are finite; a program needn't handle non-finite values.
Results may differ from the reference program's by a relative error of at most 0.018.
Values may be sent and summed in bfloat16 or wider, within the bound.
A program may use at most 64 MiB of HBM per device.

```python
import math
import jax
import jax.numpy as jnp
import numpy as np
from jax import lax

D = 4096
HEADS = 32
HD = 128
D_EXP = 2048
TOPK = 2
SEQ_DEV = 16
CACHE = 1024
KV_HEADS = 16
EXPERTS = 16
SEQS = 256
CAP = 4


def set_ends(entries, rng, least, top_value):
    shape = entries.shape
    place = [jax.random.randint(jax.random.fold_in(rng, axis), (), 0, shape[axis]) for axis in range(len(shape))]
    entries = entries.at[tuple(place)].set(least)
    longest = shape.index(max(shape))
    place[longest] = (place[longest] + 1) % shape[longest]
    return entries.at[tuple(place)].set(top_value)


def level_of(stream_key, extent, split, smallest, largest):
    level = 1.0
    for axis_at, shards_of in split:
        heights = jax.random.uniform(jax.random.fold_in(jax.random.fold_in(stream_key, 6), axis_at), (shards_of,), jnp.float32, smallest / len(split), largest / len(split))
        level = level * jnp.repeat(jnp.exp(heights), extent[axis_at] // shards_of).reshape((-1,) + (1,) * (len(extent) - 1 - axis_at))
    return level


def routed_block(key, own, number, rows, count, top, most, lean):
    order = jax.random.permutation(key, count)
    crowded, usual = portions_of(count, rows * top, most, lean, True), portions_of(count, rows * top, most, lean, False)
    places = jnp.arange(count)

    def named(tallies, rotation):
        used = int((tallies > 0).sum())
        fixed = max(1, used // 4)
        passed = fixed + (places - fixed + rotation * (used - fixed)) % max(1, count - fixed)
        return jnp.zeros((count,), jnp.int32).at[order[jnp.where(places < fixed, places, passed)]].set(jnp.asarray(tallies, jnp.int32))

    tallies = jnp.where(number % 4 == 0, named(crowded, number // 4), named(usual, number - number // 4 - 1))
    mixed = jax.random.permutation(jax.random.fold_in(own, 3), count)
    giver, taker = mixed[0:count // 2 * 2:2], mixed[1:count // 2 * 2:2]
    room = jnp.minimum(tallies[giver] - 1, most - tallies[taker]) // 2
    room = jnp.where((giver == order[0]) | (taker == order[0]) | (tallies[taker] == 0), 0, jnp.maximum(room, 0))
    passed = jax.random.randint(jax.random.fold_in(own, 4), (count // 2,), 0, 1 << 20) % (room + 1)
    tallies = tallies.at[giver].add(-passed).at[taker].add(passed)
    labels = jnp.searchsorted(jnp.cumsum(tallies), jnp.arange(rows * top), side="right").astype(jnp.int32)
    grid = labels.reshape(top, rows).T
    grid = grid[jax.random.permutation(jax.random.fold_in(own, 1), rows)]
    rotation = jax.random.randint(jax.random.fold_in(own, 2), (rows, 1), 0, top)
    return jnp.take_along_axis(grid, (jnp.arange(top)[None, :] + rotation) % top, axis=1)


def portions_of(number_of, total, limit, lean, full):
    loads = [(1 << 20) // math.isqrt(rank ** lean) + 1 for rank in range(1, number_of + 1)]
    largest = limit if full else min(limit, max(-(-total // number_of), total * loads[0] // sum(loads)))
    least = 1 if total - largest >= number_of - 1 else 0
    given, rest = [largest] + [least] * (number_of - 1), total - largest - least * (number_of - 1)
    while rest > 0:
        candidates = [i for i in range(1, number_of) if given[i] < largest] or [i for i in range(1, number_of) if given[i] < limit]
        whole, remaining = sum([loads[i] for i in candidates]), rest
        for i in candidates:
            more = min(limit - given[i], max(1, remaining * loads[i] // whole), rest)
            given[i] = given[i] + more
            rest = rest - more
    return np.array(given)


def gaussian(stream_key, shape, spread, limit, pieces=(), kind=jnp.bfloat16):
    entries = jax.random.normal(stream_key, shape, jnp.float32) * spread
    if len(pieces) > 0:
        entries = level_of(stream_key, shape, pieces, -0.22, 0.18) * entries
    return jnp.clip(entries, min=-limit, max=limit).astype(kind)


def setup_inputs(seed: int = 0) -> dict:
    arg_keys = jax.random.split(jax.random.key(seed), 19)
    hidden_in = gaussian(arg_keys[0], (SEQS, D), 1.0, 6.0, ((0, 16),))
    attn_gain = jnp.clip(1.0 + 0.18 * jax.random.normal(arg_keys[1], (D,), jnp.float32), 0.1, 1.9)
    query_weight = gaussian(arg_keys[2], (D, HEADS * HD), D ** -0.5, 0.09375, ((0, 16), (1, 16)))
    key_weight = gaussian(arg_keys[3], (D, KV_HEADS * HD), D ** -0.5, 0.09375, ((0, 16), (1, 16)))
    value_weight = gaussian(arg_keys[4], (D, KV_HEADS * HD), D ** -0.5, 0.09375, ((0, 16), (1, 16)))
    query_gain = jnp.clip(1.0 + 0.18 * jax.random.normal(arg_keys[5], (HD,), jnp.float32), 0.1, 1.9)
    key_gain = jnp.clip(1.0 + 0.18 * jax.random.normal(arg_keys[6], (HD,), jnp.float32), 0.1, 1.9)
    head_offset = jnp.clip(-7.0 + 5.0 * jax.random.uniform(arg_keys[7], (HEADS,), jnp.float32) ** level_of(arg_keys[7], (HEADS,), ((0, 16),), -0.2, 0.2), -7.0, -2.0)
    key_cache = gaussian(arg_keys[8], (SEQS, CACHE, KV_HEADS * HD), 1.0, 6.0, ((0, 16), (2, 16)))
    value_cache = gaussian(arg_keys[9], (SEQS, CACHE, KV_HEADS * HD), 1.0, 6.0, ((0, 16), (2, 16)))
    lengths = set_ends(jax.random.randint(arg_keys[10], (SEQS,), 1, CACHE + 1), jax.random.fold_in(arg_keys[10], 1), 1, CACHE).astype(jnp.int32)
    out_weight = gaussian(arg_keys[11], (HEADS * HD, D), (HEADS * HD // 16) ** -0.5, 0.375, ((0, 16), (1, 16)))
    expert_gain = jnp.clip(1.0 + 0.18 * jax.random.normal(arg_keys[12], (D,), jnp.float32), 0.1, 1.9)
    routes_keys = jax.random.split(jax.random.fold_in(arg_keys[13], 1), SEQS // SEQ_DEV)
    routes_turns = jax.random.permutation(jax.random.fold_in(arg_keys[13], 3), SEQS // SEQ_DEV)
    routes = jax.vmap(lambda own, number: routed_block(jax.random.fold_in(arg_keys[13], 2), own, number, SEQ_DEV, EXPERTS, TOPK, CAP, 1))(routes_keys, routes_turns).reshape((SEQS, TOPK))
    route_weights = jnp.clip(0.1 + 0.9 * jax.random.uniform(arg_keys[14], (SEQS, TOPK), jnp.float32) ** level_of(arg_keys[14], (SEQS, TOPK), ((0, 16),), -0.2, 0.2), 0.1, 1.0)
    gate_weight = gaussian(arg_keys[15], (EXPERTS, D, D_EXP), D ** -0.5, 0.09375, ((0, 16), (2, 16)))
    up_weight = gaussian(arg_keys[16], (EXPERTS, D, D_EXP), D ** -0.5, 0.09375, ((0, 16), (2, 16)))
    down_weight = gaussian(arg_keys[17], (EXPERTS, D_EXP, D), D_EXP ** -0.5, 0.125, ((0, 16), (1, 16)))
    return {"hidden_in": hidden_in, "attn_gain": attn_gain, "query_weight": query_weight, "key_weight": key_weight, "value_weight": value_weight, "query_gain": query_gain, "key_gain": key_gain, "head_offset": head_offset, "key_cache": key_cache, "value_cache": value_cache, "lengths": lengths, "out_weight": out_weight, "expert_gain": expert_gain, "routes": routes, "route_weights": route_weights, "gate_weight": gate_weight, "up_weight": up_weight, "down_weight": down_weight}


EPSILON = 1e-06

def norm_rows(values, gain):
    meansq = lax.optimization_barrier(jnp.mean(values * values, axis=-1, keepdims=True))
    return values * lax.rsqrt(meansq + EPSILON) * gain

def reference(hidden_in, attn_gain, query_weight, key_weight, value_weight, query_gain, key_gain, head_offset, key_cache, value_cache, lengths, out_weight, expert_gain, routes, route_weights, gate_weight, up_weight, down_weight):
    groups = HEADS // KV_HEADS
    x_float = hidden_in.astype(jnp.float32)
    normed = norm_rows(x_float, attn_gain).astype(jnp.bfloat16)
    query_raw = jnp.dot(normed, query_weight, preferred_element_type=jnp.float32).astype(jnp.bfloat16)
    key_raw = jnp.dot(normed, key_weight, preferred_element_type=jnp.float32).astype(jnp.bfloat16)
    fresh_values = jnp.dot(normed, value_weight, preferred_element_type=jnp.float32).astype(jnp.bfloat16)
    query = norm_rows(query_raw.astype(jnp.float32).reshape(SEQS, HEADS, HD), query_gain).astype(jnp.bfloat16)
    fresh_keys = norm_rows(key_raw.astype(jnp.float32).reshape(SEQS, KV_HEADS, HD), key_gain).astype(jnp.bfloat16)
    offsets = head_offset.reshape(KV_HEADS, groups)

    def attend(args):
        query_row, key_rows, value_rows, length = args
        keys = key_rows.reshape(CACHE, KV_HEADS, HD).astype(jnp.float32)
        values = value_rows.reshape(CACHE, KV_HEADS, HD).astype(jnp.float32)
        grouped = query_row.reshape(KV_HEADS, groups, HD).astype(jnp.float32)
        scores = jnp.einsum('kgd,skd->kgs', grouped, keys) * HD ** (-0.5) + offsets[:, :, None]
        live = jnp.arange(CACHE, dtype=jnp.int32)[None, None, :] < length
        breaks = jnp.where(live, jax.nn.softplus(scores), 0.0)
        suffix = lax.cumsum(breaks, axis=2, reverse=True) - breaks
        stick = jnp.where(live, jnp.exp(jax.nn.log_sigmoid(scores) - suffix), 0.0).astype(jnp.bfloat16)
        result = jnp.einsum('kgs,skd->kgd', stick.astype(jnp.float32), values)
        return result.astype(jnp.bfloat16).reshape(HEADS * HD)
    attended = lax.map(attend, (query, key_cache, value_cache, lengths))
    projected = jnp.dot(attended, out_weight, preferred_element_type=jnp.float32)
    residual = (x_float + projected).astype(jnp.bfloat16)
    expert_in = norm_rows(residual.astype(jnp.float32), expert_gain).astype(jnp.bfloat16)

    def add_expert(total, index):
        gate = jnp.dot(expert_in, gate_weight[index], preferred_element_type=jnp.float32)
        upward = jnp.dot(expert_in, up_weight[index], preferred_element_type=jnp.float32)
        hidden = (jax.nn.silu(gate) * upward).astype(jnp.bfloat16)
        output = jnp.dot(hidden, down_weight[index], preferred_element_type=jnp.float32).astype(jnp.bfloat16)
        weight = lax.optimization_barrier(jnp.sum(jnp.where(routes == index, route_weights, 0.0), axis=1))
        return (total + weight[:, None] * output.astype(jnp.float32), None)
    mixed, _ = lax.scan(add_expert, jnp.zeros((SEQS, D), jnp.float32), jnp.arange(EXPERTS, dtype=jnp.int32))
    layer_out = (residual.astype(jnp.float32) + mixed).astype(jnp.bfloat16)
    return (layer_out, fresh_keys.reshape(SEQS, KV_HEADS * HD), fresh_values)
```

```python
import functools

import jax
import jax.numpy as jnp
from jax import lax
from jax.experimental import pallas as pl
from jax.experimental.pallas import tpu as pltpu
from jax.sharding import PartitionSpec as P

EPSILON = 1e-06
MESH = pl.DeviceIdType.MESH
F32 = jnp.float32
BF16 = jnp.bfloat16
ROWS = 16
CAP = 4


def iota(shape, dim):
    return lax.broadcasted_iota(jnp.int32, shape, dim)


def pieces(v):
    hi = v.astype(BF16)
    rest = v - hi.astype(F32)
    mid = rest.astype(BF16)
    low = (rest - mid.astype(F32)).astype(BF16)
    return hi, mid, low


def dot(a, b):
    return jnp.dot(a, b, preferred_element_type=F32)


def kernel(
    n,
    x_h,
    again,
    wq_h,
    wk_h,
    wv_h,
    qg,
    kg,
    ho,
    kc_h,
    vc_h,
    lens,
    wo_h,
    eg,
    routes,
    rw,
    gw_h,
    uw_h,
    dw_h,
    out,
    fk,
    fv,
    xv,
    xn,
    xg,
    wqkv,
    part,
    pr,
    kc,
    vc,
    att,
    agb,
    wo,
    terms,
    rsb,
    xts,
    xtr,
    res_s,
    res_r,
    disp,
    dx,
    xs,
    xa,
    wgu,
    acc,
    gu,
    hid,
    ha,
    dwr,
    ybuf,
    yt,
    rt,
    tri,
    pt,
    cmb,
    geb,
    quarter,
    lsem,
    ssem,
    rsem,
    dsem,
    drsem,
):
    e = lax.axis_index("ep")
    t = lax.axis_index("tp")
    width = n * 256
    cache = kc.shape[1]

    bar = pltpu.get_barrier_semaphore()

    def greet(d, c):
        pl.semaphore_signal(bar, inc=1, device_id=(lax.rem(e + d, n), t), device_id_type=MESH)
        pl.semaphore_signal(bar, inc=1, device_id=(e, lax.rem(t + d, n)), device_id_type=MESH)
        return c

    lax.fori_loop(1, n, greet, 0)

    def load(src, dst, k):
        cp = pltpu.make_async_copy(src, dst, lsem.at[k])
        cp.start()
        return cp

    lx = load(x_h, xv, 0)
    lq = load(wq_h, wqkv.at[:, pl.ds(0, 256)], 1)
    lk = load(wk_h, wqkv.at[:, pl.ds(256, 128)], 2)
    lv = load(wv_h, wqkv.at[:, pl.ds(384, 128)], 3)
    lo = load(wo_h, wo, 4)
    lkc = load(kc_h, kc, 5)
    lvc = load(vc_h, vc, 6)
    lg = load(gw_h.at[0], wgu.at[:, pl.ds(0, 128)], 7)
    lu = load(uw_h.at[0], wgu.at[:, pl.ds(128, 128)], 8)
    t256 = pl.multiple_of(t * 256, 256)
    ld = load(dw_h.at[0, :, pl.ds(t256, 256)], dwr.at[t], 9)

    def send(k, axis, src_at, dst):
        me = e if axis == "ep" else t

        def one(d, c):
            p = lax.rem(me + d, n)
            pltpu.make_async_remote_copy(
                src_ref=src_at(p),
                dst_ref=dst,
                send_sem=ssem.at[k],
                recv_sem=rsem.at[k],
                device_id=(p, t) if axis == "ep" else (e, p),
                device_id_type=MESH,
            ).start()
            return c

        lax.fori_loop(1, n, one, 0)

    def await_all(ref, sem):
        pltpu.make_async_copy(ref, ref, sem).wait()

    lx.wait()
    x = xv[...].astype(F32)
    meansq = jnp.sum(x * x, axis=1, keepdims=True) * (1.0 / width)
    xn[...] = (x * lax.rsqrt(meansq + EPSILON) * again[...]).astype(BF16)

    tri[...] = (iota((256, 256), 0) >= iota((256, 256), 1)).astype(F32).astype(BF16)
    lane = iota((ROWS, 8 * n), 1)
    lower = (iota((ROWS, ROWS), 0) > iota((ROWS, ROWS), 1)).astype(F32).astype(BF16)

    def placed_slots(first, second):
        member = jnp.where((first == lane // 8) | (second == lane // 8), 1.0, 0.0)
        rank = dot(lower, member.astype(BF16))
        return jnp.where(rank == (lane % 4).astype(F32), member, 0.0)

    r0 = routes[:, 0:1]
    r1 = routes[:, 1:2]
    slots = placed_slots(r0, r1)
    weighted = slots * jnp.where(r0 == lane // 8, rw[:, 0:1], rw[:, 1:2])
    first_half = jnp.where((lane // 4) % 2 == 0, weighted, 0.0)
    halves = jnp.concatenate([first_half, weighted - first_half], axis=0)
    c_hi, c_mid, c_low = pieces(halves)
    cmb[pl.ds(0, 2 * ROWS), :] = c_hi
    cmb[pl.ds(2 * ROWS, 2 * ROWS), :] = c_mid
    cmb[pl.ds(4 * ROWS, 2 * ROWS), :] = c_low
    for c in range(n):
        geb[c] = jnp.where(
            iota((8, 128), 0) < 4,
            jnp.broadcast_to(eg[2 * c : 2 * c + 1, :], (8, 128)),
            jnp.broadcast_to(eg[2 * c + 1 : 2 * c + 2, :], (8, 128)),
        )
    for s in range(4):
        quarter[s] = (iota((16, 128), 0) // 4 == s).astype(F32).astype(BF16)
    xts[:, pl.ds(0, 256)] = xv[:, pl.ds(t256, 256)].astype(F32)
    lanes = iota((ROWS, 128), 1)
    xts[:, pl.ds(256, 128)] = jnp.where(
        lanes == 0, r0.astype(F32), jnp.where(lanes == 1, r1.astype(F32), 0.0)
    )

    pl.semaphore_wait(bar, 2 * (n - 1))
    e16 = pl.multiple_of(e * ROWS, ROWS)
    e256 = pl.multiple_of(e * 256, 256)
    t16 = pl.multiple_of(t * ROWS, ROWS)
    send(0, "ep", lambda p: xn.at[:, pl.ds(pl.multiple_of(p * 256, 256), 256)], xg.at[pl.ds(e16, ROWS), :])
    xg[pl.ds(e16, ROWS), :] = xn[:, pl.ds(e256, 256)]

    def spread(d, c):
        p = lax.rem(t + d, n)
        pltpu.make_async_remote_copy(
            src_ref=dw_h.at[0, :, pl.ds(pl.multiple_of(p * 256, 256), 256)],
            dst_ref=dwr.at[t],
            send_sem=dsem,
            recv_sem=drsem,
            device_id=(e, p),
            device_id_type=MESH,
        ).start()
        return c

    lax.fori_loop(1, n, spread, 0)

    lq.wait()
    lk.wait()
    lv.wait()
    await_all(xg.at[pl.ds(0, (n - 1) * ROWS), :], rsem.at[0])

    def to_mirror(src, dst, k):
        return pltpu.make_async_remote_copy(
            src_ref=src,
            dst_ref=dst,
            send_sem=ssem.at[k],
            recv_sem=rsem.at[k],
            device_id=(t, e),
            device_id_type=MESH,
        )

    part[...] = dot(xg[...], wqkv[...]).astype(BF16)
    send(1, "ep", lambda p: part.at[pl.ds(pl.multiple_of(p * ROWS, ROWS), ROWS), :], pr.at[e])
    pr[e] = part[pl.ds(e16, ROWS), :]

    @pl.when(e != t)
    def _():
        to_mirror(xts, xtr, 8).start()

    @pl.when(e == t)
    def _():
        xtr[...] = xts[...]

    await_all(pr.at[pl.ds(0, n - 1)], rsem.at[1])
    summed = pr[0].astype(F32)
    for k in range(1, n):
        summed = summed + pr[k].astype(F32)

    def head_norm(raw, gain):
        v = raw.astype(BF16).astype(F32)
        meansq = jnp.sum(v * v, axis=1, keepdims=True) * (1.0 / 128)
        return v * lax.rsqrt(meansq + EPSILON) * gain

    fk[...] = head_norm(summed[:, 256:384], kg[...]).astype(BF16)
    fv[...] = summed[:, 384:512].astype(BF16)
    query = jnp.concatenate(
        [head_norm(summed[:, 0:128], qg[...]), head_norm(summed[:, 128:256], qg[...])], axis=0
    )
    row = iota((2 * ROWS, 128), 0)
    lkc.wait()
    z = jnp.zeros((2 * ROWS, cache), F32)
    for b in range(ROWS):
        own = jnp.where(row % ROWS == b, query, 0.0).astype(BF16)
        z = z + lax.dot_general(own, kc[b], (((1,), (1,)), ((), ())), preferred_element_type=F32)
    offset = jnp.where(iota((2 * ROWS, 1), 0) < ROWS, ho[0], ho[1])
    z = z * 128**-0.5 + offset
    lens_col = jnp.sum(
        jnp.where(
            iota((2 * ROWS, ROWS), 0) % ROWS == iota((2 * ROWS, ROWS), 1), lens[...].astype(F32), 0.0
        ),
        axis=1,
        keepdims=True,
    )
    live = iota((2 * ROWS, cache), 1).astype(F32) < lens_col
    breaks = jnp.where(live, jnp.maximum(z, 0.0) + jnp.log1p(jnp.exp(-jnp.abs(z))), 0.0)
    chunks = cache // 256
    parts = pieces(breaks)
    stacked = jnp.concatenate(
        [p[:, c * 256 : (c + 1) * 256] for p in parts for c in range(chunks)], axis=0
    )
    sums = dot(stacked, tri[...])
    size = chunks * 2 * ROWS
    sums = sums[:size] + sums[size : 2 * size] + sums[2 * size :]
    after = jnp.zeros((2 * ROWS, 1), F32)
    suffix = [None] * chunks
    for c in range(chunks - 1, -1, -1):
        here = sums[c * 2 * ROWS : (c + 1) * 2 * ROWS]
        suffix[c] = here + after
        after = after + here[:, 0:1]
    suffix = jnp.concatenate(suffix, axis=1)
    stick = jnp.where(live, jnp.exp(z - suffix), 0.0)
    lvc.wait()
    wide_row = iota((2 * ROWS, cache), 0)
    attended = jnp.zeros((2 * ROWS, 128), F32)
    for b in range(ROWS):
        own = jnp.where(wide_row % ROWS == b, stick, 0.0).astype(BF16)
        attended = attended + dot(own, vc[b])
    att[:, pl.ds(0, 128)] = attended[:ROWS].astype(BF16)
    att[:, pl.ds(128, 128)] = attended[ROWS:].astype(BF16)

    send(2, "ep", lambda p: att, agb.at[pl.ds(e16, ROWS), :])
    agb[pl.ds(e16, ROWS), :] = att[...]

    @pl.when(e != t)
    def _():
        to_mirror(xts, xtr, 8).wait_recv()

    theirs = placed_slots(xtr[:, 256:257].astype(jnp.int32), xtr[:, 257:258].astype(jnp.int32))
    pt[...] = jnp.transpose(theirs, (1, 0)).astype(BF16)

    lo.wait()
    await_all(agb.at[pl.ds(0, (n - 1) * ROWS), :], rsem.at[2])

    terms[...] = dot(agb[...], wo[...]).astype(BF16)
    send(3, "tp", lambda p: terms.at[pl.ds(pl.multiple_of(p * ROWS, ROWS), ROWS), :], rsb.at[t])
    rsb[t] = terms[pl.ds(t16, ROWS), :]
    await_all(rsb.at[pl.ds(0, n - 1)], rsem.at[3])
    projected = rsb[0].astype(F32)
    for k in range(1, n):
        projected = projected + rsb[k].astype(F32)
    residual = (xtr[:, pl.ds(0, 256)] + projected).astype(BF16)
    res_s[...] = residual

    picked = dot(pt[...], residual)
    disp[...] = jnp.where(
        (iota((8 * n, 128), 0) // 4) % 2 == 0, picked[:, 0:128], picked[:, 128:256]
    )
    send(4, "ep", lambda p: disp.at[pl.ds(pl.multiple_of(p * 8, 8), 8), :], dx.at[e])
    dx[e] = disp[pl.ds(pl.multiple_of(e * 8, 8), 8), :]

    @pl.when(e != t)
    def _():
        to_mirror(res_s, res_r, 9).start()

    @pl.when(e == t)
    def _():
        res_r[...] = res_s[...]

    await_all(dx.at[pl.ds(0, n - 1)], rsem.at[4])

    v = dx[...]
    squares = jnp.sum(jnp.sum(v * v, axis=0), axis=1, keepdims=True)
    squares = jnp.broadcast_to(squares, (8, 128))
    squares = squares + pltpu.roll(squares, 4, 0)
    scale = lax.rsqrt(squares * (1.0 / width) + EPSILON)
    xs[...] = (v * scale[None] * geb[...]).reshape(n // 2, 16, 128).astype(BF16)
    send(5, "tp", lambda p: xs, xa.at[t])
    xa[t] = xs[...]
    lg.wait()
    lu.wait()
    await_all(xa.at[pl.ds(0, n - 1)], rsem.at[5])

    total = jnp.zeros((n * 16, 256), F32)
    for c in range(n // 2):
        block = xa[:, c]
        lhs = jnp.concatenate(
            [(block * quarter[s][None]).reshape(n * 16, 128) for s in range(4)], axis=1
        )
        total = total + dot(lhs, wgu[pl.ds(c * 512, 512), :])
    acc[...] = total
    for b in range(n):
        gu[pl.ds(b * 4, 4), :] = (
            acc[pl.ds(b * 16, 4), :]
            + acc[pl.ds(b * 16 + 4, 4), :]
            + acc[pl.ds(b * 16 + 8, 4), :]
            + acc[pl.ds(b * 16 + 12, 4), :]
        )
    gate = gu[:, 0:128]
    hid[...] = (gate * jax.nn.sigmoid(gate) * gu[:, 128:256]).astype(BF16)

    send(6, "tp", lambda p: hid, ha.at[t])
    ha[t] = hid[...]
    ld.wait()
    await_all(dwr.at[pl.ds(0, n - 1)], drsem)
    await_all(ha.at[pl.ds(0, n - 1)], rsem.at[6])
    y = jnp.zeros((4 * n, 256), F32)
    for k in range(0, n, 2):
        lhs = jnp.concatenate([ha[k], ha[k + 1]], axis=1)
        y = y + dot(lhs, dwr[pl.ds(k, 2)].reshape(256, 256))
    ybuf[...] = y.astype(BF16).astype(F32)
    for b in range(n):
        yt[pl.ds(b * 8, 4), :] = ybuf[pl.ds(b * 4, 4), pl.ds(0, 128)]
        yt[pl.ds(b * 8 + 4, 4), :] = ybuf[pl.ds(b * 4, 4), pl.ds(128, 128)]

    send(7, "ep", lambda p: yt.at[pl.ds(pl.multiple_of(p * 8, 8), 8), :], rt.at[e])
    rt[e] = yt[pl.ds(pl.multiple_of(e * 8, 8), 8), :]

    @pl.when(e != t)
    def _():
        to_mirror(res_s, res_r, 9).wait_recv()

    await_all(rt.at[pl.ds(0, n - 1)], rsem.at[7])
    back = rt[...].reshape(8 * n, 128).astype(BF16)
    mixed = dot(cmb[...], back)
    mixed = mixed[0 : 2 * ROWS] + mixed[2 * ROWS : 4 * ROWS] + mixed[4 * ROWS :]
    mixed = jnp.concatenate([mixed[:ROWS], mixed[ROWS:]], axis=1)
    out[...] = (res_r[...].astype(F32) + mixed).astype(BF16)

    await_all(xg.at[pl.ds(0, (n - 1) * ROWS), :], ssem.at[0])
    await_all(pr.at[pl.ds(0, n - 1)], ssem.at[1])
    await_all(agb.at[pl.ds(0, (n - 1) * ROWS), :], ssem.at[2])
    await_all(rsb.at[pl.ds(0, n - 1)], ssem.at[3])
    await_all(dx.at[pl.ds(0, n - 1)], ssem.at[4])
    await_all(xa.at[pl.ds(0, n - 1)], ssem.at[5])
    await_all(ha.at[pl.ds(0, n - 1)], ssem.at[6])
    await_all(rt.at[pl.ds(0, n - 1)], ssem.at[7])
    await_all(dwr.at[pl.ds(0, n - 1)], dsem)

    @pl.when(e != t)
    def _():
        to_mirror(xts, xtr, 8).wait_send()
        to_mirror(res_s, res_r, 9).wait_send()


def body(
    hidden_in,
    attn_gain,
    query_weight,
    key_weight,
    value_weight,
    query_gain,
    key_gain,
    head_offset,
    key_cache,
    value_cache,
    lengths,
    out_weight,
    expert_gain,
    routes,
    route_weights,
    gate_weight,
    up_weight,
    down_weight,
):
    n = lax.axis_size("ep")
    width = hidden_in.shape[1]
    cache = key_cache.shape[1]
    vmem = pl.BlockSpec(memory_space=pltpu.VMEM)
    hbm = pl.BlockSpec(memory_space=pl.ANY)
    smem = pl.BlockSpec(memory_space=pltpu.SMEM)
    V = pltpu.VMEM
    scratch = [
        V((ROWS, width), BF16),
        V((ROWS, width), BF16),
        V((n * ROWS, 256), BF16),
        V((256, 512), BF16),
        V((n * ROWS, 512), BF16),
        V((n, ROWS, 512), BF16),
        V((ROWS, cache, 128), BF16),
        V((ROWS, cache, 128), BF16),
        V((ROWS, 256), BF16),
        V((n * ROWS, 256), BF16),
        V((256, 256), BF16),
        V((n * ROWS, 256), BF16),
        V((n, ROWS, 256), BF16),
        V((ROWS, 384), F32),
        V((ROWS, 384), F32),
        V((ROWS, 256), BF16),
        V((ROWS, 256), BF16),
        V((8 * n, 128), F32),
        V((n, 8, 128), F32),
        V((n // 2, 16, 128), BF16),
        V((n, n // 2, 16, 128), BF16),
        V((width, 256), BF16),
        V((n * 16, 256), F32),
        V((n * 4, 256), F32),
        V((n * 4, 128), BF16),
        V((n, n * 4, 128), BF16),
        V((n, 128, 256), BF16),
        V((n * 4, 256), F32),
        V((8 * n, 128), F32),
        V((n, 8, 128), F32),
        V((256, 256), BF16),
        V((8 * n, ROWS), BF16),
        V((6 * ROWS, 8 * n), BF16),
        V((n, 8, 128), F32),
        V((4, 16, 128), BF16),
        pltpu.SemaphoreType.DMA((10,)),
        pltpu.SemaphoreType.DMA((10,)),
        pltpu.SemaphoreType.DMA((10,)),
        pltpu.SemaphoreType.DMA,
        pltpu.SemaphoreType.DMA,
    ]
    return pl.pallas_call(
        functools.partial(kernel, n),
        out_shape=(
            jax.ShapeDtypeStruct((ROWS, 256), BF16),
            jax.ShapeDtypeStruct((ROWS, 128), BF16),
            jax.ShapeDtypeStruct((ROWS, 128), BF16),
        ),
        in_specs=[hbm, vmem, hbm, hbm, hbm, vmem, vmem, smem, hbm, hbm, vmem, hbm]
        + [vmem, vmem, vmem, hbm, hbm, hbm],
        out_specs=(vmem, vmem, vmem),
        scratch_shapes=scratch,
        compiler_params=pltpu.CompilerParams(
            collective_id=0, has_side_effects=True, vmem_limit_bytes=60 * 1024 * 1024
        ),
    )(
        hidden_in,
        attn_gain.reshape(1, width),
        query_weight,
        key_weight,
        value_weight,
        query_gain.reshape(1, 128),
        key_gain.reshape(1, 128),
        head_offset,
        key_cache,
        value_cache,
        lengths.reshape(1, ROWS),
        out_weight,
        expert_gain.reshape(width // 128, 128),
        routes,
        route_weights,
        gate_weight,
        up_weight,
        down_weight,
    )


def solution(mesh):
    placed = (
        P("ep", None),
        P(),
        P("ep", "tp"),
        P("ep", "tp"),
        P("ep", "tp"),
        P(),
        P(),
        P("tp"),
        P("ep", None, "tp"),
        P("ep", None, "tp"),
        P("ep"),
        P("tp", "ep"),
        P(),
        P("ep", None),
        P("ep", None),
        P("ep", None, "tp"),
        P("ep", None, "tp"),
        P("ep", "tp", None),
    )
    return jax.shard_map(
        body,
        mesh=mesh,
        in_specs=placed,
        out_specs=(P("ep", "tp"), P("ep", "tp"), P("ep", "tp")),
        check_vma=False,
    )
```

```python
import functools
import math

import jax
import jax.numpy as jnp
from jax import lax
from jax.experimental import pallas as pl
from jax.experimental.pallas import tpu as pltpu
from jax.sharding import PartitionSpec as P

EPSILON = 1e-06
MESH = pl.DeviceIdType.MESH
F32 = jnp.float32
BF16 = jnp.bfloat16
ROWS = 16
CAP = 4


def iota(shape, dim):
    return lax.broadcasted_iota(jnp.int32, shape, dim)


def pieces(v):
    hi = v.astype(BF16)
    rest = v - hi.astype(F32)
    mid = rest.astype(BF16)
    low = (rest - mid.astype(F32)).astype(BF16)
    return hi, mid, low


def dot(a, b):
    return jnp.dot(a, b, preferred_element_type=F32)


def plane_steps(n):
    side = math.isqrt(n)
    steps = [(dy, dx) for dy in range(side) for dx in range(side) if (dy, dx) != (0, 0)]
    return sorted(steps, key=lambda s: -sum(min(d, side - d) for d in s))


def column_steps(n):
    deep = n // 2
    steps = [(dz, dc) for dz in range(deep) for dc in range(2) if (dz, dc) != (0, 0)]
    return sorted(steps, key=lambda s: -min(s[0], deep - s[0]))


def kernel(
    n,
    x_h,
    again_h,
    wq_h,
    wk_h,
    wv_h,
    qg_h,
    kg_h,
    ho_h,
    kc_h,
    vc_h,
    lens_h,
    wo_h,
    eg_h,
    routes_h,
    rw_h,
    gw_h,
    uw_h,
    dw_h,
    out,
    fk,
    fv,
    again,
    qg,
    kg,
    ho,
    lens,
    eg,
    routes,
    rw,
    xv,
    xn,
    xg,
    wqkv,
    partq,
    partk,
    prq,
    prk,
    kc,
    vc,
    att,
    agb,
    wo,
    terms,
    rsb,
    xts,
    xtr,
    res_s,
    res_r,
    disp,
    xd,
    wgu,
    dwp,
    ys,
    rt,
    tri,
    pt,
    cmb,
    geb,
    lsem,
    ssem,
    rsem,
    bsend,
    brecv,
):
    e = lax.axis_index("ep")
    t = lax.axis_index("tp")
    side = math.isqrt(n)
    deep = n // 2
    ey, ex = e // side, lax.rem(e, side)
    tz, core = t // 2, lax.rem(t, 2)
    width = n * 256
    cache = kc.shape[1]

    def in_plane(step):
        return lax.rem(ey + step[0], side) * side + lax.rem(ex + step[1], side)

    def in_column(step):
        return lax.rem(tz + step[0], deep) * 2 + lax.rem(core + step[1], 2)

    bar = pltpu.get_barrier_semaphore()
    for step in plane_steps(n):
        pl.semaphore_signal(bar, inc=1, device_id=(in_plane(step), t), device_id_type=MESH)
    for step in column_steps(n):
        pl.semaphore_signal(bar, inc=1, device_id=(e, in_column(step)), device_id_type=MESH)

    def load(src, dst, k):
        cp = pltpu.make_async_copy(src, dst, lsem.at[k])
        cp.start()
        return cp

    mine256 = pl.multiple_of(core * 256, 128)
    lx = load(x_h, xv, 0)
    small = [load(a, b, 11 + i) for i, (a, b) in enumerate([(again_h, again), (qg_h, qg), (kg_h, kg), (ho_h, ho), (lens_h, lens), (eg_h, eg), (routes_h, routes), (rw_h, rw)])]
    lq = load(wq_h, wqkv.at[:, pl.ds(0, 256)], 1)
    lk = load(wk_h, wqkv.at[:, pl.ds(256, 128)], 2)
    lv = load(wv_h, wqkv.at[:, pl.ds(384, 128)], 3)
    lo = load(wo_h, wo, 4)
    lkc = load(kc_h, kc, 5)
    lvc = load(vc_h, vc, 6)
    lg = load(gw_h.at[0], wgu.at[:, pl.ds(mine256, 128)], 7)
    lu = load(uw_h.at[0], wgu.at[:, pl.ds(pl.multiple_of(mine256 + 128, 128), 128)], 8)
    ld = load(dw_h.at[0], dwp.at[core], 9)

    def remote(src, dst, k, dev, s=ssem, r=rsem):
        return pltpu.make_async_remote_copy(
            src_ref=src,
            dst_ref=dst,
            send_sem=s.at[k],
            recv_sem=r.at[k],
            device_id=dev,
            device_id_type=MESH,
        )

    def rows_of(p, size=ROWS):
        return pl.ds(pl.multiple_of(p * size, size), size)

    def cols_of(p, size=256):
        return pl.ds(pl.multiple_of(p * size, size), size)

    def await_all(ref, sem):
        pltpu.make_async_copy(ref, ref, sem).wait()

    lx.wait()
    for cp in small:
        cp.wait()
    x = xv[...].astype(F32)
    meansq = jnp.sum(x * x, axis=1, keepdims=True) * (1.0 / width)
    xn[...] = (x * lax.rsqrt(meansq + EPSILON) * again[...]).astype(BF16)

    tri[...] = (iota((256, 256), 0) >= iota((256, 256), 1)).astype(F32).astype(BF16)
    lane = iota((ROWS, 8 * n), 1)
    lower = (iota((ROWS, ROWS), 0) > iota((ROWS, ROWS), 1)).astype(F32).astype(BF16)
    diagonal = iota((ROWS, ROWS), 0) == iota((ROWS, ROWS), 1)

    def column(line):
        return jnp.sum(jnp.where(diagonal, line, 0.0), axis=1, keepdims=True)

    expert = (lane // 8).astype(F32)

    def placed_slots(first, second):
        member = jnp.where((first == expert) | (second == expert), 1.0, 0.0)
        rank = dot(lower, member.astype(BF16))
        return jnp.where(rank == (lane % 4).astype(F32), member, 0.0)

    r0 = column(routes[0:1, :].astype(F32))
    r1 = column(routes[1:2, :].astype(F32))
    slots = placed_slots(r0, r1)
    weighted = slots * jnp.where(r0 == expert, column(rw[0:1, :]), column(rw[1:2, :]))
    first_half = jnp.where((lane // 4) % 2 == 0, weighted, 0.0)
    halves = jnp.concatenate([first_half, weighted - first_half], axis=0)
    c_hi, c_mid, c_low = pieces(halves)
    cmb[pl.ds(0, 2 * ROWS), :] = c_hi
    cmb[pl.ds(2 * ROWS, 2 * ROWS), :] = c_mid
    cmb[pl.ds(4 * ROWS, 2 * ROWS), :] = c_low
    for c in range(n):
        geb[c] = jnp.where(
            iota((8, 128), 0) < 4,
            jnp.broadcast_to(eg[2 * c : 2 * c + 1, :], (8, 128)),
            jnp.broadcast_to(eg[2 * c + 1 : 2 * c + 2, :], (8, 128)),
        )
    xts[:, pl.ds(0, 256)] = xv[:, cols_of(t)].astype(F32)
    lanes = iota((ROWS, 128), 1)
    xts[:, pl.ds(256, 128)] = jnp.where(lanes == 0, r0, jnp.where(lanes == 1, r1, 0.0))

    pl.semaphore_wait(bar, 2 * (n - 1))
    for step in plane_steps(n):
        p = in_plane(step)
        remote(xn.at[:, cols_of(p)], xg.at[rows_of(e), :], 0, (p, t)).start()
    xg[rows_of(e), :] = xn[:, cols_of(e)]
    lq.wait()
    lk.wait()
    lv.wait()
    others = pl.ds(0, n - 1)
    other_rows = pl.ds(0, (n - 1) * ROWS)
    await_all(xg.at[other_rows, :], rsem.at[0])

    partq[...] = dot(xg[...], wqkv[:, pl.ds(0, 256)]).astype(BF16)
    for step in plane_steps(n):
        p = in_plane(step)
        remote(partq.at[rows_of(p), :], prq.at[e], 1, (p, t)).start()
    prq[e] = partq[rows_of(e), :]
    partk[...] = dot(xg[...], wqkv[:, pl.ds(256, 256)]).astype(BF16)
    for step in plane_steps(n):
        p = in_plane(step)
        remote(partk.at[rows_of(p), :], prk.at[e], 2, (p, t)).start()
    prk[e] = partk[rows_of(e), :]

    @pl.when(e != t)
    def _():
        remote(xts, xtr, 3, (t, e)).start()

    @pl.when(e == t)
    def _():
        xtr[...] = xts[...]

    def head_norm(raw, gain):
        v = raw.astype(BF16).astype(F32)
        meansq = jnp.sum(v * v, axis=1, keepdims=True) * (1.0 / 128)
        return v * lax.rsqrt(meansq + EPSILON) * gain

    def added(ref):
        total = ref[0].astype(F32)
        for k in range(1, n):
            total = total + ref[k].astype(F32)
        return total

    await_all(prq.at[others], rsem.at[1])

    other = (e, tz * 2 + 1 - core)
    swaps = [
        remote(gw_h.at[0], wgu.at[:, pl.ds(mine256, 128)], 0, other, bsend, brecv),
        remote(
            uw_h.at[0],
            wgu.at[:, pl.ds(pl.multiple_of(mine256 + 128, 128), 128)],
            1,
            other,
            bsend,
            brecv,
        ),
        remote(dw_h.at[0], dwp.at[core], 2, other, bsend, brecv),
    ]
    for cp in swaps:
        cp.start()

    summed = added(prq)
    query = jnp.concatenate(
        [head_norm(summed[:, 0:128], qg[...]), head_norm(summed[:, 128:256], qg[...])], axis=0
    )
    row = iota((2 * ROWS, 128), 0)
    lkc.wait()
    z = jnp.zeros((2 * ROWS, cache), F32)
    for b in range(ROWS):
        own = jnp.where(row % ROWS == b, query, 0.0).astype(BF16)
        z = z + lax.dot_general(own, kc[b], (((1,), (1,)), ((), ())), preferred_element_type=F32)
    offset = jnp.where(iota((2 * ROWS, 1), 0) < ROWS, ho[0:1, 0:1], ho[0:1, 1:2])
    z = z * 128**-0.5 + offset
    lens_col = jnp.sum(
        jnp.where(
            iota((2 * ROWS, ROWS), 0) % ROWS == iota((2 * ROWS, ROWS), 1), lens[...].astype(F32), 0.0
        ),
        axis=1,
        keepdims=True,
    )
    live = iota((2 * ROWS, cache), 1).astype(F32) < lens_col
    breaks = jnp.where(live, jnp.maximum(z, 0.0) + jnp.log1p(jnp.exp(-jnp.abs(z))), 0.0)
    chunks = cache // 256
    parts = pieces(breaks)
    stacked = jnp.concatenate(
        [p[:, c * 256 : (c + 1) * 256] for p in parts for c in range(chunks)], axis=0
    )
    sums = dot(stacked, tri[...])
    size = chunks * 2 * ROWS
    sums = sums[:size] + sums[size : 2 * size] + sums[2 * size :]
    after = jnp.zeros((2 * ROWS, 1), F32)
    suffix = [None] * chunks
    for c in range(chunks - 1, -1, -1):
        here = sums[c * 2 * ROWS : (c + 1) * 2 * ROWS]
        suffix[c] = here + after
        after = after + here[:, 0:1]
    suffix = jnp.concatenate(suffix, axis=1)
    stick = jnp.where(live, jnp.exp(z - suffix), 0.0)
    lvc.wait()
    wide_row = iota((2 * ROWS, cache), 0)
    attended = jnp.zeros((2 * ROWS, 128), F32)
    for b in range(ROWS):
        own = jnp.where(wide_row % ROWS == b, stick, 0.0).astype(BF16)
        attended = attended + dot(own, vc[b])
    att[:, pl.ds(0, 128)] = attended[:ROWS].astype(BF16)
    att[:, pl.ds(128, 128)] = attended[ROWS:].astype(BF16)

    for step in plane_steps(n):
        remote(att, agb.at[rows_of(e), :], 4, (in_plane(step), t)).start()
    agb[rows_of(e), :] = att[...]

    await_all(prk.at[others], rsem.at[2])
    summed = added(prk)
    fk[...] = head_norm(summed[:, 0:128], kg[...]).astype(BF16)
    fv[...] = summed[:, 128:256].astype(BF16)

    @pl.when(e != t)
    def _():
        remote(xts, xtr, 3, (t, e)).wait_recv()

    theirs = placed_slots(xtr[:, 256:257], xtr[:, 257:258])
    pt[...] = jnp.transpose(theirs, (1, 0)).astype(BF16)

    lo.wait()
    await_all(agb.at[other_rows, :], rsem.at[4])

    terms[...] = dot(agb[...], wo[...]).astype(BF16)
    for step in column_steps(n):
        p = in_column(step)
        remote(terms.at[rows_of(p), :], rsb.at[t], 5, (e, p)).start()
    rsb[t] = terms[rows_of(t), :]
    await_all(rsb.at[others], rsem.at[5])
    residual = (xtr[:, pl.ds(0, 256)] + added(rsb)).astype(BF16)
    res_s[...] = residual

    picked = dot(pt[...], residual)
    half = (iota((8 * n, 128), 0) // 4) % 2
    disp[...] = (
        jnp.where(half == 0, picked[:, 0:128], picked[:, 128:256]).reshape(n, 8, 128).astype(BF16)
    )

    def dispatch(dz):
        there = lax.rem(tz + dz, deep) * 2 + core
        for step in plane_steps(n):
            p = in_plane(step)
            remote(disp.at[p], xd.at[tz * n + e], 6, (p, there)).start()
        return there

    def dispatch_far(i, c):
        there = dispatch(deep // 2 + (i + 1) // 2 * (2 * lax.rem(i, 2) - 1))
        remote(disp.at[e], xd.at[tz * n + e], 6, (e, there)).start()
        return c

    lax.fori_loop(0, deep - 1, dispatch_far, 0)
    dispatch(0)
    xd[tz * n + e] = disp[e]

    @pl.when(e != t)
    def _():
        remote(res_s, res_r, 7, (t, e)).start()

    @pl.when(e == t)
    def _():
        res_r[...] = res_s[...]

    lg.wait()
    lu.wait()
    swaps[0].wait_recv()
    swaps[1].wait_recv()

    all_but_one = pl.ds(0, deep * n - 1)
    await_all(xd.at[all_but_one], rsem.at[6])

    squares = jnp.zeros((deep, 8, 128), F32)
    arrived = xd[...].reshape(deep, n, 8, 128)
    for c in range(n):
        v = arrived[:, c].astype(F32)
        squares = squares + v * v
    squares = jnp.sum(squares, axis=2, keepdims=True)
    squares = jnp.broadcast_to(squares, (deep, 8, 128)).reshape(deep * 8, 128)

    def both_halves(v):
        return jnp.concatenate(
            [v[i * 8 : i * 8 + 8] + pltpu.roll(v[i * 8 : i * 8 + 8], 4, 0) for i in range(deep)], axis=0
        )

    scale = lax.rsqrt(both_halves(squares) * (1.0 / width) + EPSILON)
    first = (iota((deep * 8, 128), 0) // 4) % 2 == 0
    total = jnp.zeros((deep * 8, 512), F32)
    for c in range(n):
        v = (arrived[:, c].astype(F32) * geb[c][None]).reshape(deep * 8, 128)
        v = v * scale
        lhs = jnp.concatenate([jnp.where(first, v, 0.0), jnp.where(first, 0.0, v)], axis=1)
        total = total + dot(lhs.astype(BF16), wgu[pl.ds(c * 256, 256), :])
    total = both_halves(total)
    hidden = []
    for k in range(2):
        gate = total[:, k * 256 : k * 256 + 128]
        hidden.append(gate * jax.nn.sigmoid(gate) * total[:, k * 256 + 128 : k * 256 + 256])
    hidden = jnp.concatenate(hidden, axis=1)
    wide_first = (iota((deep * 8, 256), 0) // 4) % 2 == 0
    hidden0 = jnp.where(wide_first, hidden, 0.0).astype(BF16)
    hidden1 = jnp.where(wide_first, 0.0, hidden).astype(BF16)
    ld.wait()
    swaps[2].wait_recv()
    down = dwp[...].reshape(256, width)
    for c in range(n):
        y = dot(hidden0, down[:, c * 256 : c * 256 + 128]) + dot(
            hidden1, down[:, c * 256 + 128 : c * 256 + 256]
        )
        ys[:, c] = y.reshape(deep, 8, 128).astype(BF16)

    def give_back(dz, dc, skip):
        there = lax.rem(tz + dz, deep) * 2 + lax.rem(core + dc, 2)
        for i in range(deep):
            b = 2 * i + core
            cp = remote(ys.at[i, there], rt.at[tz * n + e], 8, (b, there))
            if not skip:
                cp.start()
                continue

            @pl.when(b != e)
            def _():
                cp.start()

            @pl.when(b == e)
            def _():
                rt[tz * n + e] = ys[i, there]

    def give_far(i, c):
        dz = deep // 2 + (i + 1) // 2 * (2 * lax.rem(i, 2) - 1)
        give_back(dz, 0, False)
        give_back(dz, 1, False)
        return c

    lax.fori_loop(0, deep - 1, give_far, 0)
    give_back(0, 1, False)
    give_back(0, 0, True)

    @pl.when(e != t)
    def _():
        remote(res_s, res_r, 7, (t, e)).wait_recv()

    def await_returned(sem):
        @pl.when(lax.rem(e, 2) != core)
        def _():
            await_all(rt, sem)

        @pl.when(lax.rem(e, 2) == core)
        def _():
            await_all(rt.at[all_but_one], sem)

    await_returned(rsem.at[8])
    back = rt[pl.ds(0, n)].astype(F32)
    for k in range(1, deep):
        back = back + rt[pl.ds(k * n, n)].astype(F32)
    mixed = dot(cmb[...], back.reshape(8 * n, 128).astype(BF16))
    mixed = mixed[0 : 2 * ROWS] + mixed[2 * ROWS : 4 * ROWS] + mixed[4 * ROWS :]
    mixed = jnp.concatenate([mixed[:ROWS], mixed[ROWS:]], axis=1)
    out[...] = (res_r[...].astype(F32) + mixed).astype(BF16)

    await_all(xg.at[other_rows, :], ssem.at[0])
    await_all(prq.at[others], ssem.at[1])
    await_all(prk.at[others], ssem.at[2])
    await_all(agb.at[other_rows, :], ssem.at[4])
    await_all(rsb.at[others], ssem.at[5])
    await_all(xd.at[all_but_one], ssem.at[6])
    await_returned(ssem.at[8])
    for cp in swaps:
        cp.wait_send()

    @pl.when(e != t)
    def _():
        remote(xts, xtr, 3, (t, e)).wait_send()
        remote(res_s, res_r, 7, (t, e)).wait_send()


def emit(a, b, c, a_out, b_out, c_out):
    a_out[...] = a[...]
    b_out[...] = b[...]
    c_out[...] = c[...]


def body(
    hidden_in,
    attn_gain,
    query_weight,
    key_weight,
    value_weight,
    query_gain,
    key_gain,
    head_offset,
    key_cache,
    value_cache,
    lengths,
    out_weight,
    expert_gain,
    routes,
    route_weights,
    gate_weight,
    up_weight,
    down_weight,
):
    n = lax.axis_size("ep")
    width = hidden_in.shape[1]
    cache = key_cache.shape[1]
    vmem = pl.BlockSpec(memory_space=pltpu.VMEM)
    hbm = pl.BlockSpec(memory_space=pl.ANY)
    V = pltpu.VMEM
    I32 = jnp.int32
    deep = n // 2
    scratch = [
        V((1, width), F32),
        V((1, 128), F32),
        V((1, 128), F32),
        V((1, 2), F32),
        V((1, ROWS), I32),
        V((width // 128, 128), F32),
        V((2, ROWS), I32),
        V((2, ROWS), F32),
        V((ROWS, width), BF16),
        V((ROWS, width), BF16),
        V((n * ROWS, 256), BF16),
        V((256, 512), BF16),
        V((n * ROWS, 256), BF16),
        V((n * ROWS, 256), BF16),
        V((n, ROWS, 256), BF16),
        V((n, ROWS, 256), BF16),
        V((ROWS, cache, 128), BF16),
        V((ROWS, cache, 128), BF16),
        V((ROWS, 256), BF16),
        V((n * ROWS, 256), BF16),
        V((256, 256), BF16),
        V((n * ROWS, 256), BF16),
        V((n, ROWS, 256), BF16),
        V((ROWS, 384), F32),
        V((ROWS, 384), F32),
        V((ROWS, 256), BF16),
        V((ROWS, 256), BF16),
        V((n, 8, 128), BF16),
        V((deep * n, 8, 128), BF16),
        V((width, 512), BF16),
        V((2, 128, width), BF16),
        V((deep, n, 8, 128), BF16),
        V((deep * n, 8, 128), BF16),
        V((256, 256), BF16),
        V((8 * n, ROWS), BF16),
        V((6 * ROWS, 8 * n), BF16),
        V((n, 8, 128), F32),
        pltpu.SemaphoreType.DMA((20,)),
        pltpu.SemaphoreType.DMA((9,)),
        pltpu.SemaphoreType.DMA((9,)),
        pltpu.SemaphoreType.DMA((3,)),
        pltpu.SemaphoreType.DMA((3,)),
    ]
    results = (
        jax.ShapeDtypeStruct((ROWS, 256), BF16),
        jax.ShapeDtypeStruct((ROWS, 128), BF16),
        jax.ShapeDtypeStruct((ROWS, 128), BF16),
    )
    made = pl.pallas_call(
        functools.partial(kernel, n),
        out_shape=results,
        in_specs=[hbm] * 18,
        out_specs=(vmem, vmem, vmem),
        scratch_shapes=scratch,
        compiler_params=pltpu.CompilerParams(
            collective_id=0, has_side_effects=True, vmem_limit_bytes=60 * 1024 * 1024
        ),
    )(
        hidden_in,
        attn_gain.reshape(1, width),
        query_weight,
        key_weight,
        value_weight,
        query_gain.reshape(1, 128),
        key_gain.reshape(1, 128),
        head_offset.reshape(1, 2),
        key_cache,
        value_cache,
        lengths.reshape(1, ROWS),
        out_weight,
        expert_gain.reshape(width // 128, 128),
        routes.T,
        route_weights.T,
        gate_weight,
        up_weight,
        down_weight,
    )
    return pl.pallas_call(
        emit, out_shape=results, in_specs=[vmem] * 3, out_specs=(vmem, vmem, vmem)
    )(*made)


def solution(mesh):
    placed = (
        P("ep", None),
        P(),
        P("ep", "tp"),
        P("ep", "tp"),
        P("ep", "tp"),
        P(),
        P(),
        P("tp"),
        P("ep", None, "tp"),
        P("ep", None, "tp"),
        P("ep"),
        P("tp", "ep"),
        P(),
        P("ep", None),
        P("ep", None),
        P("ep", None, "tp"),
        P("ep", None, "tp"),
        P("ep", "tp", None),
    )
    return jax.shard_map(
        body,
        mesh=mesh,
        in_specs=placed,
        out_specs=(P("ep", "tp"), P("ep", "tp"), P("ep", "tp")),
        check_vma=False,
    )
```

```python
import functools
import math

import jax
import jax.numpy as jnp
from jax import lax
from jax.experimental import pallas as pl
from jax.experimental.pallas import tpu as pltpu
from jax.sharding import PartitionSpec as P

EPSILON = 1e-06
MESH = pl.DeviceIdType.MESH
F32 = jnp.float32
BF16 = jnp.bfloat16
ROWS = 16
CAP = 4


def iota(shape, dim):
    return lax.broadcasted_iota(jnp.int32, shape, dim)


def pieces(v):
    hi = v.astype(BF16)
    rest = v - hi.astype(F32)
    mid = rest.astype(BF16)
    low = (rest - mid.astype(F32)).astype(BF16)
    return hi, mid, low


def dot(a, b):
    return jnp.dot(a, b, preferred_element_type=F32)


def plane_steps(n):
    side = math.isqrt(n)
    steps = [(dy, dx) for dy in range(side) for dx in range(side) if (dy, dx) != (0, 0)]
    return sorted(steps, key=lambda s: -sum(min(d, side - d) for d in s))


def column_steps(n):
    deep = n // 2
    steps = [(dz, dc) for dz in range(deep) for dc in range(2) if (dz, dc) != (0, 0)]
    return sorted(steps, key=lambda s: -min(s[0], deep - s[0]))


def kernel(
    n,
    x_h,
    again_h,
    wq_h,
    wk_h,
    wv_h,
    qg_h,
    kg_h,
    ho_h,
    kc_h,
    vc_h,
    lens_h,
    wo_h,
    eg_h,
    routes_h,
    rw_h,
    gw_h,
    uw_h,
    dw_h,
    out,
    fk,
    fv,
    again,
    qg,
    kg,
    ho,
    lens,
    eg,
    routes,
    rw,
    xv,
    xn,
    xg,
    wqkv,
    partq,
    partk,
    prq,
    prk,
    kc,
    vc,
    att,
    agb,
    wo,
    terms,
    rsb,
    xts,
    xtr,
    res_s,
    res_r,
    disp,
    xd,
    wgu,
    dwp,
    ys,
    rt,
    tri,
    pt,
    cmb,
    geb,
    lsem,
    ssem,
    rsem,
    bsend,
    brecv,
):
    e = lax.axis_index("ep")
    t = lax.axis_index("tp")
    side = math.isqrt(n)
    deep = n // 2
    ey, ex = e // side, lax.rem(e, side)
    tz, core = t // 2, lax.rem(t, 2)
    width = n * 256
    cache = kc.shape[1]

    def in_plane(step):
        return lax.rem(ey + step[0], side) * side + lax.rem(ex + step[1], side)

    shift = lax.rem(core + ex, 2)
    parity_steps = sorted(
        [(dy, m) for dy in range(side) for m in range(side // 2)],
        key=lambda s: (-min(s[0], side - s[0]), -s[1]),
    )

    def of_parity(step):
        return lax.rem(ey + step[0], side) * side + lax.rem(ex + shift + 2 * step[1], side)

    same = lax.rem(e, 2) == core
    unlike = lax.rem(e, 2) != core

    def in_column(step):
        return lax.rem(tz + step[0], deep) * 2 + lax.rem(core + step[1], 2)

    bar = pltpu.get_barrier_semaphore()
    for step in plane_steps(n):
        pl.semaphore_signal(bar, inc=1, device_id=(in_plane(step), t), device_id_type=MESH)
    for step in column_steps(n):
        pl.semaphore_signal(bar, inc=1, device_id=(e, in_column(step)), device_id_type=MESH)

    def load(src, dst, k):
        cp = pltpu.make_async_copy(src, dst, lsem.at[k])
        cp.start()
        return cp

    mine256 = pl.multiple_of(core * 256, 256)
    lx = load(x_h, xv, 0)
    small = [load(a, b, 11 + i) for i, (a, b) in enumerate([(again_h, again), (qg_h, qg), (kg_h, kg), (ho_h, ho), (lens_h, lens), (eg_h, eg), (routes_h, routes), (rw_h, rw)])]
    at_q = wqkv.at[:, pl.ds(mine256, 256)]
    at_k = wqkv.at[:, pl.ds(pl.multiple_of(mine256 + 512, 128), 128)]
    at_v = wqkv.at[:, pl.ds(pl.multiple_of(mine256 + 640, 128), 128)]
    at_o = wo.at[pl.ds(pl.multiple_of(core * 256, 256), 256), :]
    lq = load(wq_h, at_q, 1)
    lk = load(wk_h, at_k, 2)
    lv = load(wv_h, at_v, 3)
    lo = load(wo_h, at_o, 4)
    lkc = load(kc_h, kc, 5)
    lvc = load(vc_h, vc, 6)
    lg = load(gw_h.at[0], wgu.at[:, pl.ds(mine256, 128)], 7)
    lu = load(uw_h.at[0], wgu.at[:, pl.ds(pl.multiple_of(mine256 + 128, 128), 128)], 8)
    ld = load(dw_h.at[0], dwp.at[core], 9)

    def remote(src, dst, k, dev, s=ssem, r=rsem):
        return pltpu.make_async_remote_copy(
            src_ref=src,
            dst_ref=dst,
            send_sem=s.at[k],
            recv_sem=r.at[k],
            device_id=dev,
            device_id_type=MESH,
        )

    def rows_of(p, size=ROWS):
        return pl.ds(pl.multiple_of(p * size, size), size)

    def cols_of(p, size=256):
        return pl.ds(pl.multiple_of(p * size, size), size)

    def await_all(ref, sem):
        pltpu.make_async_copy(ref, ref, sem).wait()

    lx.wait()
    for cp in small:
        cp.wait()
    x = xv[...].astype(F32)
    meansq = jnp.sum(x * x, axis=1, keepdims=True) * (1.0 / width)
    xn[...] = (x * lax.rsqrt(meansq + EPSILON) * again[...]).astype(BF16)

    tri[...] = (iota((256, 256), 0) >= iota((256, 256), 1)).astype(F32).astype(BF16)
    lane = iota((ROWS, 8 * n), 1)
    lower = (iota((ROWS, ROWS), 0) > iota((ROWS, ROWS), 1)).astype(F32).astype(BF16)
    diagonal = iota((ROWS, ROWS), 0) == iota((ROWS, ROWS), 1)

    def column(line):
        return jnp.sum(jnp.where(diagonal, line, 0.0), axis=1, keepdims=True)

    expert = (lane // 8).astype(F32)

    def placed_slots(first, second):
        member = jnp.where((first == expert) | (second == expert), 1.0, 0.0)
        rank = dot(lower, member.astype(BF16))
        return jnp.where(rank == (lane % 4).astype(F32), member, 0.0)

    r0 = column(routes[0:1, :].astype(F32))
    r1 = column(routes[1:2, :].astype(F32))
    slots = placed_slots(r0, r1)
    weighted = slots * jnp.where(r0 == expert, column(rw[0:1, :]), column(rw[1:2, :]))
    first_half = jnp.where((lane // 4) % 2 == 0, weighted, 0.0)
    halves = jnp.concatenate([first_half, weighted - first_half], axis=0)
    c_hi, c_mid, c_low = pieces(halves)
    cmb[pl.ds(0, 2 * ROWS), :] = c_hi
    cmb[pl.ds(2 * ROWS, 2 * ROWS), :] = c_mid
    cmb[pl.ds(4 * ROWS, 2 * ROWS), :] = c_low
    for c in range(n):
        geb[c] = jnp.where(
            iota((8, 128), 0) < 4,
            jnp.broadcast_to(eg[2 * c : 2 * c + 1, :], (8, 128)),
            jnp.broadcast_to(eg[2 * c + 1 : 2 * c + 2, :], (8, 128)),
        )
    xts[:, pl.ds(0, 256)] = xv[:, cols_of(t)].astype(F32)
    lanes = iota((ROWS, 128), 1)
    xts[:, pl.ds(256, 128)] = jnp.where(lanes == 0, r0, jnp.where(lanes == 1, r1, 0.0))

    pl.semaphore_wait(bar, 2 * (n - 1))

    @pl.when(same)
    def _():
        for step in plane_steps(n):
            p = in_plane(step)
            remote(xn.at[:, cols_of(p)], xg.at[rows_of(e // 2), :], 0, (p, t)).start()
        xg[rows_of(e // 2), :] = xn[:, cols_of(e)]

    other = (e, tz * 2 + 1 - core)
    swaps = [
        remote(wq_h, at_q, 0, other, bsend, brecv),
        remote(wk_h, at_k, 1, other, bsend, brecv),
        remote(wv_h, at_v, 2, other, bsend, brecv),
        remote(wo_h, at_o, 3, other, bsend, brecv),
    ]
    for cp in swaps:
        cp.start()
    others = pl.ds(0, n - 1)

    def await_blocks(ref, sem, count):
        @pl.when(same)
        def _():
            await_all(ref.at[pl.ds(0, count - 1)], sem)

        @pl.when(unlike)
        def _():
            await_all(ref, sem)

    lq.wait()
    swaps[0].wait_recv()

    @pl.when(same)
    def _():
        await_all(xg.at[pl.ds(0, (deep - 1) * ROWS), :], rsem.at[0])

    @pl.when(unlike)
    def _():
        await_all(xg, rsem.at[0])

    def to_owners(part, dst, k):
        for step in parity_steps:
            b = of_parity(step)
            for dc in (1, 0):
                there = lax.rem(core + dc, 2)
                cp = remote(part.at[rows_of(b // 2), cols_of(there)], dst.at[e], k, (b, tz * 2 + there))
                if step != (0, 0) or dc == 1:
                    cp.start()
                    continue

                @pl.when(unlike)
                def _():
                    cp.start()

                @pl.when(same)
                def _():
                    dst[e] = part[rows_of(e // 2), cols_of(core)]

    partq[...] = dot(xg[...], wqkv[:, pl.ds(0, 512)]).astype(BF16)
    to_owners(partq, prq, 1)
    lk.wait()
    lv.wait()
    swaps[1].wait_recv()
    swaps[2].wait_recv()
    partk[...] = dot(xg[...], wqkv[:, pl.ds(512, 512)]).astype(BF16)
    to_owners(partk, prk, 2)

    @pl.when(e != t)
    def _():
        remote(xts, xtr, 3, (t, e)).start()

    @pl.when(e == t)
    def _():
        xtr[...] = xts[...]

    def head_norm(raw, gain):
        v = raw.astype(BF16).astype(F32)
        meansq = jnp.sum(v * v, axis=1, keepdims=True) * (1.0 / 128)
        return v * lax.rsqrt(meansq + EPSILON) * gain

    def added(ref):
        total = ref[0].astype(F32)
        for k in range(1, ref.shape[0]):
            total = total + ref[k].astype(F32)
        return total

    await_blocks(prq, rsem.at[1], n)

    experts = [
        remote(gw_h.at[0], wgu.at[:, pl.ds(mine256, 128)], 4, other, bsend, brecv),
        remote(
            uw_h.at[0],
            wgu.at[:, pl.ds(pl.multiple_of(mine256 + 128, 128), 128)],
            5,
            other,
            bsend,
            brecv,
        ),
        remote(dw_h.at[0], dwp.at[core], 6, other, bsend, brecv),
    ]
    for cp in experts:
        cp.start()

    summed = added(prq)
    query = jnp.concatenate(
        [head_norm(summed[:, 0:128], qg[...]), head_norm(summed[:, 128:256], qg[...])], axis=0
    )
    row = iota((2 * ROWS, 128), 0)
    lkc.wait()
    z = jnp.zeros((2 * ROWS, cache), F32)
    for b in range(ROWS):
        own = jnp.where(row % ROWS == b, query, 0.0).astype(BF16)
        z = z + lax.dot_general(own, kc[b], (((1,), (1,)), ((), ())), preferred_element_type=F32)
    offset = jnp.where(iota((2 * ROWS, 1), 0) < ROWS, ho[0:1, 0:1], ho[0:1, 1:2])
    z = z * 128**-0.5 + offset
    lens_col = jnp.sum(
        jnp.where(
            iota((2 * ROWS, ROWS), 0) % ROWS == iota((2 * ROWS, ROWS), 1), lens[...].astype(F32), 0.0
        ),
        axis=1,
        keepdims=True,
    )
    live = iota((2 * ROWS, cache), 1).astype(F32) < lens_col
    breaks = jnp.where(live, jnp.maximum(z, 0.0) + jnp.log1p(jnp.exp(-jnp.abs(z))), 0.0)
    chunks = cache // 256
    parts = pieces(breaks)
    stacked = jnp.concatenate(
        [p[:, c * 256 : (c + 1) * 256] for p in parts for c in range(chunks)], axis=0
    )
    sums = dot(stacked, tri[...])
    size = chunks * 2 * ROWS
    sums = sums[:size] + sums[size : 2 * size] + sums[2 * size :]
    after = jnp.zeros((2 * ROWS, 1), F32)
    suffix = [None] * chunks
    for c in range(chunks - 1, -1, -1):
        here = sums[c * 2 * ROWS : (c + 1) * 2 * ROWS]
        suffix[c] = here + after
        after = after + here[:, 0:1]
    suffix = jnp.concatenate(suffix, axis=1)
    stick = jnp.where(live, jnp.exp(z - suffix), 0.0)
    lvc.wait()
    wide_row = iota((2 * ROWS, cache), 0)
    attended = jnp.zeros((2 * ROWS, 128), F32)
    for b in range(ROWS):
        own = jnp.where(wide_row % ROWS == b, stick, 0.0).astype(BF16)
        attended = attended + dot(own, vc[b])
    att[:, pl.ds(0, 128)] = attended[:ROWS].astype(BF16)
    att[:, pl.ds(128, 128)] = attended[ROWS:].astype(BF16)

    heads = agb.at[rows_of(e // 2), cols_of(core)]
    keeper = tz * 2 + lax.rem(e, 2)
    for step in plane_steps(n):
        remote(att, heads, 4, (in_plane(step), keeper)).start()

    @pl.when(unlike)
    def _():
        remote(att, heads, 4, other).start()

    @pl.when(same)
    def _():
        agb[rows_of(e // 2), cols_of(core)] = att[...]

    await_blocks(prk, rsem.at[2], n)
    summed = added(prk)
    fk[...] = head_norm(summed[:, 0:128], kg[...]).astype(BF16)
    fv[...] = summed[:, 128:256].astype(BF16)

    @pl.when(e != t)
    def _():
        remote(xts, xtr, 3, (t, e)).wait_recv()

    theirs = placed_slots(xtr[:, 256:257], xtr[:, 257:258])
    pt[...] = jnp.transpose(theirs, (1, 0)).astype(BF16)

    lo.wait()
    swaps[3].wait_recv()
    await_blocks(prq, rsem.at[4], n)

    terms[...] = dot(agb[...], wo[...]).astype(BF16)
    for dz in sorted(range(1, deep), key=lambda d: -min(d, deep - d)):
        there = lax.rem(tz + dz, deep)
        remote(terms.at[rows_of(there), :], rsb.at[tz], 5, (e, there * 2 + core)).start()
    rsb[tz] = terms[rows_of(tz), :]
    await_all(rsb.at[pl.ds(0, deep - 1)], rsem.at[5])
    residual = (xtr[:, pl.ds(0, 256)] + added(rsb)).astype(BF16)
    res_s[...] = residual

    picked = dot(pt[...], residual)
    half = (iota((8 * n, 128), 0) // 4) % 2
    disp[...] = (
        jnp.where(half == 0, picked[:, 0:128], picked[:, 128:256]).reshape(n, 8, 128).astype(BF16)
    )

    def dispatch(dz):
        there = lax.rem(tz + dz, deep) * 2 + core
        for step in plane_steps(n):
            p = in_plane(step)
            remote(disp.at[p], xd.at[tz * n + e], 6, (p, there)).start()
        return there

    def dispatch_far(i, c):
        there = dispatch(deep // 2 + (i + 1) // 2 * (2 * lax.rem(i, 2) - 1))
        remote(disp.at[e], xd.at[tz * n + e], 6, (e, there)).start()
        return c

    lax.fori_loop(0, deep - 1, dispatch_far, 0)
    dispatch(0)
    xd[tz * n + e] = disp[e]

    @pl.when(e != t)
    def _():
        remote(res_s, res_r, 7, (t, e)).start()

    @pl.when(e == t)
    def _():
        res_r[...] = res_s[...]

    lg.wait()
    lu.wait()
    experts[0].wait_recv()
    experts[1].wait_recv()

    all_but_one = pl.ds(0, deep * n - 1)
    await_all(xd.at[all_but_one], rsem.at[6])

    squares = jnp.zeros((deep, 8, 128), F32)
    arrived = xd[...].reshape(deep, n, 8, 128)
    for c in range(n):
        v = arrived[:, c].astype(F32)
        squares = squares + v * v
    squares = jnp.sum(squares, axis=2, keepdims=True)
    squares = jnp.broadcast_to(squares, (deep, 8, 128)).reshape(deep * 8, 128)

    def both_halves(v):
        return jnp.concatenate(
            [v[i * 8 : i * 8 + 8] + pltpu.roll(v[i * 8 : i * 8 + 8], 4, 0) for i in range(deep)], axis=0
        )

    scale = lax.rsqrt(both_halves(squares) * (1.0 / width) + EPSILON)
    first = (iota((deep * 8, 128), 0) // 4) % 2 == 0
    total = jnp.zeros((deep * 8, 512), F32)
    for c in range(n):
        v = (arrived[:, c].astype(F32) * geb[c][None]).reshape(deep * 8, 128)
        v = v * scale
        lhs = jnp.concatenate([jnp.where(first, v, 0.0), jnp.where(first, 0.0, v)], axis=1)
        total = total + dot(lhs.astype(BF16), wgu[pl.ds(c * 256, 256), :])
    total = both_halves(total)
    hidden = []
    for k in range(2):
        gate = total[:, k * 256 : k * 256 + 128]
        hidden.append(gate * jax.nn.sigmoid(gate) * total[:, k * 256 + 128 : k * 256 + 256])
    hidden = jnp.concatenate(hidden, axis=1)
    wide_first = (iota((deep * 8, 256), 0) // 4) % 2 == 0
    hidden0 = jnp.where(wide_first, hidden, 0.0).astype(BF16)
    hidden1 = jnp.where(wide_first, 0.0, hidden).astype(BF16)
    ld.wait()
    experts[2].wait_recv()
    down = dwp[...].reshape(256, width)
    for c in range(n):
        y = dot(hidden0, down[:, c * 256 : c * 256 + 128]) + dot(
            hidden1, down[:, c * 256 + 128 : c * 256 + 256]
        )
        ys[:, c] = y.reshape(deep, 8, 128).astype(BF16)

    def give_back(dz, dc, skip):
        there = lax.rem(tz + dz, deep) * 2 + lax.rem(core + dc, 2)
        for i in range(deep):
            b = 2 * i + core
            cp = remote(ys.at[i, there], rt.at[tz * n + e], 8, (b, there))
            if not skip:
                cp.start()
                continue

            @pl.when(b != e)
            def _():
                cp.start()

            @pl.when(b == e)
            def _():
                rt[tz * n + e] = ys[i, there]

    def give_far(i, c):
        dz = deep // 2 + (i + 1) // 2 * (2 * lax.rem(i, 2) - 1)
        give_back(dz, 0, False)
        give_back(dz, 1, False)
        return c

    lax.fori_loop(0, deep - 1, give_far, 0)
    give_back(0, 1, False)
    give_back(0, 0, True)

    @pl.when(e != t)
    def _():
        remote(res_s, res_r, 7, (t, e)).wait_recv()

    await_blocks(rt, rsem.at[8], deep * n)
    back = rt[pl.ds(0, n)].astype(F32)
    for k in range(1, deep):
        back = back + rt[pl.ds(k * n, n)].astype(F32)
    mixed = dot(cmb[...], back.reshape(8 * n, 128).astype(BF16))
    mixed = mixed[0 : 2 * ROWS] + mixed[2 * ROWS : 4 * ROWS] + mixed[4 * ROWS :]
    mixed = jnp.concatenate([mixed[:ROWS], mixed[ROWS:]], axis=1)
    out[...] = (res_r[...].astype(F32) + mixed).astype(BF16)

    @pl.when(same)
    def _():
        await_all(xn.at[:, pl.ds(0, (n - 1) * 256)], ssem.at[0])

    await_blocks(prq, ssem.at[1], n)
    await_blocks(prk, ssem.at[2], n)
    await_blocks(prq, ssem.at[4], n)
    await_all(rsb.at[pl.ds(0, deep - 1)], ssem.at[5])
    await_all(xd.at[all_but_one], ssem.at[6])
    await_blocks(rt, ssem.at[8], deep * n)
    for cp in swaps + experts:
        cp.wait_send()

    @pl.when(e != t)
    def _():
        remote(xts, xtr, 3, (t, e)).wait_send()
        remote(res_s, res_r, 7, (t, e)).wait_send()


def emit(a, b, c, a_out, b_out, c_out):
    a_out[...] = a[...]
    b_out[...] = b[...]
    c_out[...] = c[...]


def body(
    hidden_in,
    attn_gain,
    query_weight,
    key_weight,
    value_weight,
    query_gain,
    key_gain,
    head_offset,
    key_cache,
    value_cache,
    lengths,
    out_weight,
    expert_gain,
    routes,
    route_weights,
    gate_weight,
    up_weight,
    down_weight,
):
    n = lax.axis_size("ep")
    width = hidden_in.shape[1]
    cache = key_cache.shape[1]
    vmem = pl.BlockSpec(memory_space=pltpu.VMEM)
    hbm = pl.BlockSpec(memory_space=pltpu.HBM)
    V = pltpu.VMEM
    I32 = jnp.int32
    deep = n // 2
    scratch = [
        V((1, width), F32),
        V((1, 128), F32),
        V((1, 128), F32),
        V((1, 2), F32),
        V((1, ROWS), I32),
        V((width // 128, 128), F32),
        V((2, ROWS), I32),
        V((2, ROWS), F32),
        V((ROWS, width), BF16),
        V((ROWS, width), BF16),
        V((deep * ROWS, 256), BF16),
        V((256, 1024), BF16),
        V((deep * ROWS, 512), BF16),
        V((deep * ROWS, 512), BF16),
        V((n, ROWS, 256), BF16),
        V((n, ROWS, 256), BF16),
        V((ROWS, cache, 128), BF16),
        V((ROWS, cache, 128), BF16),
        V((ROWS, 256), BF16),
        V((deep * ROWS, 512), BF16),
        V((512, 256), BF16),
        V((deep * ROWS, 256), BF16),
        V((deep, ROWS, 256), BF16),
        V((ROWS, 384), F32),
        V((ROWS, 384), F32),
        V((ROWS, 256), BF16),
        V((ROWS, 256), BF16),
        V((n, 8, 128), BF16),
        V((deep * n, 8, 128), BF16),
        V((width, 512), BF16),
        V((2, 128, width), BF16),
        V((deep, n, 8, 128), BF16),
        V((deep * n, 8, 128), BF16),
        V((256, 256), BF16),
        V((8 * n, ROWS), BF16),
        V((6 * ROWS, 8 * n), BF16),
        V((n, 8, 128), F32),
        pltpu.SemaphoreType.DMA((20,)),
        pltpu.SemaphoreType.DMA((9,)),
        pltpu.SemaphoreType.DMA((9,)),
        pltpu.SemaphoreType.DMA((7,)),
        pltpu.SemaphoreType.DMA((7,)),
    ]
    results = (
        jax.ShapeDtypeStruct((ROWS, 256), BF16),
        jax.ShapeDtypeStruct((ROWS, 128), BF16),
        jax.ShapeDtypeStruct((ROWS, 128), BF16),
    )
    made = pl.pallas_call(
        functools.partial(kernel, n),
        out_shape=tuple(V(r.shape, r.dtype) for r in results),
        in_specs=[hbm] * 18,
        out_specs=(vmem, vmem, vmem),
        scratch_shapes=scratch,
        compiler_params=pltpu.CompilerParams(
            collective_id=0, has_side_effects=True, vmem_limit_bytes=60 * 1024 * 1024
        ),
    )(
        hidden_in,
        attn_gain.reshape(1, width),
        query_weight,
        key_weight,
        value_weight,
        query_gain.reshape(1, 128),
        key_gain.reshape(1, 128),
        head_offset.reshape(1, 2),
        key_cache,
        value_cache,
        lengths.reshape(1, ROWS),
        out_weight,
        expert_gain.reshape(width // 128, 128),
        routes.T,
        route_weights.T,
        gate_weight,
        up_weight,
        down_weight,
    )
    return pl.pallas_call(
        emit, out_shape=results, in_specs=[vmem] * 3, out_specs=(vmem, vmem, vmem)
    )(*[pltpu.with_memory_space_constraint(m, pltpu.VMEM) for m in made])


def solution(mesh):
    placed = (
        P("ep", None),
        P(),
        P("ep", "tp"),
        P("ep", "tp"),
        P("ep", "tp"),
        P(),
        P(),
        P("tp"),
        P("ep", None, "tp"),
        P("ep", None, "tp"),
        P("ep"),
        P("tp", "ep"),
        P(),
        P("ep", None),
        P("ep", None),
        P("ep", None, "tp"),
        P("ep", None, "tp"),
        P("ep", "tp", None),
    )
    return jax.shard_map(
        body,
        mesh=mesh,
        in_specs=placed,
        out_specs=(P("ep", "tp"), P("ep", "tp"), P("ep", "tp")),
        check_vma=False,
    )
```

```python
import functools
import math

import jax
import jax.numpy as jnp
from jax import lax
from jax.experimental import pallas as pl
from jax.experimental.pallas import tpu as pltpu
from jax.sharding import PartitionSpec as P

EPSILON = 1e-06
MESH = pl.DeviceIdType.MESH
F32 = jnp.float32
BF16 = jnp.bfloat16
ROWS = 16
CAP = 4


def iota(shape, dim):
    return lax.broadcasted_iota(jnp.int32, shape, dim)


def pieces(v):
    hi = v.astype(BF16)
    rest = v - hi.astype(F32)
    mid = rest.astype(BF16)
    low = (rest - mid.astype(F32)).astype(BF16)
    return hi, mid, low


def dot(a, b):
    return jnp.dot(a, b, preferred_element_type=F32)


def plane_steps(n):
    side = math.isqrt(n)
    steps = [(dy, dx) for dy in range(side) for dx in range(side) if (dy, dx) != (0, 0)]
    return sorted(steps, key=lambda s: -sum(min(d, side - d) for d in s))


def column_steps(n):
    deep = n // 2
    steps = [(dz, dc) for dz in range(deep) for dc in range(2) if (dz, dc) != (0, 0)]
    return sorted(steps, key=lambda s: -min(s[0], deep - s[0]))


def kernel(
    n,
    x_h,
    again_h,
    wq_h,
    wk_h,
    wv_h,
    qg_h,
    kg_h,
    ho_h,
    kc_h,
    vc_h,
    lens_h,
    wo_h,
    eg_h,
    routes_h,
    rw_h,
    gw_h,
    uw_h,
    dw_h,
    out,
    fk,
    fv,
    again,
    qg,
    kg,
    ho,
    lens,
    eg,
    routes,
    rw,
    xv,
    xn,
    xg,
    wqkv,
    partq,
    partk,
    prq,
    prk,
    kc,
    vc,
    att,
    agb,
    wo,
    terms,
    rsb,
    xts,
    xtr,
    res_s,
    res_r,
    disp,
    xd,
    wgu,
    dwp,
    ys,
    rt,
    tri,
    pt,
    cmb,
    geb,
    lsem,
    ssem,
    rsem,
    bsend,
    brecv,
):
    e = lax.axis_index("ep")
    t = lax.axis_index("tp")
    side = math.isqrt(n)
    deep = n // 2
    ey, ex = e // side, lax.rem(e, side)
    tz, core = t // 2, lax.rem(t, 2)
    width = n * 256
    cache = kc.shape[1]

    def in_plane(step):
        return lax.rem(ey + step[0], side) * side + lax.rem(ex + step[1], side)

    shift = lax.rem(core + ex, 2)
    parity_steps = sorted(
        [(dy, m) for dy in range(side) for m in range(side // 2)],
        key=lambda s: (-min(s[0], side - s[0]), -s[1]),
    )

    def of_parity(step):
        return lax.rem(ey + step[0], side) * side + lax.rem(ex + shift + 2 * step[1], side)

    same = lax.rem(e, 2) == core
    unlike = lax.rem(e, 2) != core

    def in_column(step):
        return lax.rem(tz + step[0], deep) * 2 + lax.rem(core + step[1], 2)

    bar = pltpu.get_barrier_semaphore()
    for step in plane_steps(n):
        pl.semaphore_signal(bar, inc=1, device_id=(in_plane(step), t), device_id_type=MESH)
    for step in column_steps(n):
        pl.semaphore_signal(bar, inc=1, device_id=(e, in_column(step)), device_id_type=MESH)

    def load(src, dst, k):
        cp = pltpu.make_async_copy(src, dst, lsem.at[k])
        cp.start()
        return cp

    mine256 = pl.multiple_of(core * 256, 256)
    lx = load(x_h, xv, 0)
    small = [load(a, b, 11 + i) for i, (a, b) in enumerate([(again_h, again), (qg_h, qg), (kg_h, kg), (ho_h, ho), (lens_h, lens), (eg_h, eg), (routes_h, routes), (rw_h, rw)])]
    at_q = wqkv.at[:, pl.ds(mine256, 256)]
    at_k = wqkv.at[:, pl.ds(pl.multiple_of(mine256 + 512, 128), 128)]
    at_v = wqkv.at[:, pl.ds(pl.multiple_of(mine256 + 640, 128), 128)]
    at_o = wo.at[pl.ds(pl.multiple_of(core * 256, 256), 256), :]
    lq = load(wq_h, at_q, 1)
    lk = load(wk_h, at_k, 2)
    lv = load(wv_h, at_v, 3)
    lo = load(wo_h, at_o, 4)
    lkc = load(kc_h, kc, 5)
    lvc = load(vc_h, vc, 6)
    lg = load(gw_h.at[0], wgu.at[:, pl.ds(mine256, 128)], 7)
    lu = load(uw_h.at[0], wgu.at[:, pl.ds(pl.multiple_of(mine256 + 128, 128), 128)], 8)
    ld = load(dw_h.at[0], dwp.at[core], 9)

    def remote(src, dst, k, dev, s=ssem, r=rsem):
        return pltpu.make_async_remote_copy(
            src_ref=src,
            dst_ref=dst,
            send_sem=s.at[k],
            recv_sem=r.at[k],
            device_id=dev,
            device_id_type=MESH,
        )

    def rows_of(p, size=ROWS):
        return pl.ds(pl.multiple_of(p * size, size), size)

    def cols_of(p, size=256):
        return pl.ds(pl.multiple_of(p * size, size), size)

    def await_all(ref, sem):
        pltpu.make_async_copy(ref, ref, sem).wait()

    lx.wait()
    for cp in small:
        cp.wait()
    x = xv[...].astype(F32)
    meansq = jnp.sum(x * x, axis=1, keepdims=True) * (1.0 / width)
    xn[...] = (x * lax.rsqrt(meansq + EPSILON) * again[...]).astype(BF16)

    tri[...] = (iota((256, 256), 0) >= iota((256, 256), 1)).astype(F32).astype(BF16)
    lane = iota((ROWS, 8 * n), 1)
    lower = (iota((ROWS, ROWS), 0) > iota((ROWS, ROWS), 1)).astype(F32).astype(BF16)
    diagonal = iota((ROWS, ROWS), 0) == iota((ROWS, ROWS), 1)

    def column(line):
        return jnp.sum(jnp.where(diagonal, line, 0.0), axis=1, keepdims=True)

    expert = (lane // 8).astype(F32)

    def placed_slots(first, second):
        member = jnp.where((first == expert) | (second == expert), 1.0, 0.0)
        rank = dot(lower, member.astype(BF16))
        return jnp.where(rank == (lane % 4).astype(F32), member, 0.0)

    r0 = column(routes[0:1, :].astype(F32))
    r1 = column(routes[1:2, :].astype(F32))
    slots = placed_slots(r0, r1)
    weighted = slots * jnp.where(r0 == expert, column(rw[0:1, :]), column(rw[1:2, :]))
    first_half = jnp.where((lane // 4) % 2 == 0, weighted, 0.0)
    halves = jnp.concatenate([first_half, weighted - first_half], axis=0)
    c_hi, c_mid, c_low = pieces(halves)
    cmb[pl.ds(0, 2 * ROWS), :] = c_hi
    cmb[pl.ds(2 * ROWS, 2 * ROWS), :] = c_mid
    cmb[pl.ds(4 * ROWS, 2 * ROWS), :] = c_low
    for c in range(n):
        geb[c] = jnp.where(
            iota((8, 128), 0) < 4,
            jnp.broadcast_to(eg[2 * c : 2 * c + 1, :], (8, 128)),
            jnp.broadcast_to(eg[2 * c + 1 : 2 * c + 2, :], (8, 128)),
        )
    xts[:, pl.ds(0, 256)] = xv[:, cols_of(t)].astype(F32)
    lanes = iota((ROWS, 128), 1)
    xts[:, pl.ds(256, 128)] = jnp.where(lanes == 0, r0, jnp.where(lanes == 1, r1, 0.0))

    pl.semaphore_wait(bar, 2 * (n - 1))

    keeper = tz * 2 + lax.rem(e, 2)

    @pl.when(same)
    def _():
        for step in plane_steps(n):
            p = in_plane(step)
            remote(xn.at[:, cols_of(p)], xg.at[rows_of(e // 2), :], 0, (p, t)).start()
        xg[rows_of(e // 2), :] = xn[:, cols_of(e)]

    other = (e, tz * 2 + 1 - core)
    swaps = [
        remote(wq_h, at_q, 0, other, bsend, brecv),
        remote(wk_h, at_k, 1, other, bsend, brecv),
        remote(wv_h, at_v, 2, other, bsend, brecv),
        remote(wo_h, at_o, 3, other, bsend, brecv),
    ]
    for cp in swaps:
        cp.start()
    others = pl.ds(0, n - 1)

    def await_blocks(ref, sem, count):
        @pl.when(same)
        def _():
            await_all(ref.at[pl.ds(0, count - 1)], sem)

        @pl.when(unlike)
        def _():
            await_all(ref, sem)

    lq.wait()
    swaps[0].wait_recv()

    @pl.when(same)
    def _():
        await_all(xg.at[pl.ds(0, (deep - 1) * ROWS), :], rsem.at[0])

    @pl.when(unlike)
    def _():
        await_all(xg, rsem.at[0])

    def to_owners(part, dst, k):
        for step in parity_steps:
            b = of_parity(step)
            for dc in (1, 0):
                there = lax.rem(core + dc, 2)
                cp = remote(part.at[rows_of(b // 2), cols_of(there)], dst.at[e], k, (b, tz * 2 + there))
                if step != (0, 0) or dc == 1:
                    cp.start()
                    continue

                @pl.when(unlike)
                def _():
                    cp.start()

                @pl.when(same)
                def _():
                    dst[e] = part[rows_of(e // 2), cols_of(core)]

    partq[...] = dot(xg[...], wqkv[:, pl.ds(0, 512)]).astype(BF16)
    to_owners(partq, prq, 1)
    lk.wait()
    lv.wait()
    swaps[1].wait_recv()
    swaps[2].wait_recv()
    partk[...] = dot(xg[...], wqkv[:, pl.ds(512, 512)]).astype(BF16)
    to_owners(partk, prk, 2)

    @pl.when(e != t)
    def _():
        remote(xts, xtr, 3, (t, e)).start()

    @pl.when(e == t)
    def _():
        xtr[...] = xts[...]

    def head_norm(raw, gain):
        v = raw.astype(BF16).astype(F32)
        meansq = jnp.sum(v * v, axis=1, keepdims=True) * (1.0 / 128)
        return v * lax.rsqrt(meansq + EPSILON) * gain

    def added(ref):
        total = ref[0].astype(F32)
        for k in range(1, ref.shape[0]):
            total = total + ref[k].astype(F32)
        return total

    await_blocks(prq, rsem.at[1], n)

    experts = [
        remote(gw_h.at[0], wgu.at[:, pl.ds(mine256, 128)], 4, other, bsend, brecv),
        remote(
            uw_h.at[0],
            wgu.at[:, pl.ds(pl.multiple_of(mine256 + 128, 128), 128)],
            5,
            other,
            bsend,
            brecv,
        ),
        remote(dw_h.at[0], dwp.at[core], 6, other, bsend, brecv),
    ]
    for cp in experts:
        cp.start()

    summed = added(prq)
    query = jnp.concatenate(
        [head_norm(summed[:, 0:128], qg[...]), head_norm(summed[:, 128:256], qg[...])], axis=0
    )
    row = iota((2 * ROWS, 128), 0)
    lkc.wait()
    z = jnp.zeros((2 * ROWS, cache), F32)
    for b in range(ROWS):
        own = jnp.where(row % ROWS == b, query, 0.0).astype(BF16)
        z = z + lax.dot_general(own, kc[b], (((1,), (1,)), ((), ())), preferred_element_type=F32)
    offset = jnp.where(iota((2 * ROWS, 1), 0) < ROWS, ho[0:1, 0:1], ho[0:1, 1:2])
    z = z * 128**-0.5 + offset
    lens_col = jnp.sum(
        jnp.where(
            iota((2 * ROWS, ROWS), 0) % ROWS == iota((2 * ROWS, ROWS), 1), lens[...].astype(F32), 0.0
        ),
        axis=1,
        keepdims=True,
    )
    live = iota((2 * ROWS, cache), 1).astype(F32) < lens_col
    breaks = jnp.where(live, jnp.maximum(z, 0.0) + jnp.log1p(jnp.exp(-jnp.abs(z))), 0.0)
    chunks = cache // 256
    parts = pieces(breaks)
    stacked = jnp.concatenate(
        [p[:, c * 256 : (c + 1) * 256] for p in parts for c in range(chunks)], axis=0
    )
    sums = dot(stacked, tri[...])
    size = chunks * 2 * ROWS
    sums = sums[:size] + sums[size : 2 * size] + sums[2 * size :]
    after = jnp.zeros((2 * ROWS, 1), F32)
    suffix = [None] * chunks
    for c in range(chunks - 1, -1, -1):
        here = sums[c * 2 * ROWS : (c + 1) * 2 * ROWS]
        suffix[c] = here + after
        after = after + here[:, 0:1]
    suffix = jnp.concatenate(suffix, axis=1)
    stick = jnp.where(live, jnp.exp(z - suffix), 0.0)
    lvc.wait()
    wide_row = iota((2 * ROWS, cache), 0)
    attended = jnp.zeros((2 * ROWS, 128), F32)
    for b in range(ROWS):
        own = jnp.where(wide_row % ROWS == b, stick, 0.0).astype(BF16)
        attended = attended + dot(own, vc[b])
    att[:, pl.ds(0, 128)] = attended[:ROWS].astype(BF16)
    att[:, pl.ds(128, 128)] = attended[ROWS:].astype(BF16)

    heads = agb.at[rows_of(e // 2), cols_of(core)]
    for step in plane_steps(n):
        remote(att, heads, 4, (in_plane(step), keeper)).start()

    @pl.when(unlike)
    def _():
        remote(att, heads, 4, other).start()

    @pl.when(same)
    def _():
        agb[rows_of(e // 2), cols_of(core)] = att[...]

    await_blocks(prk, rsem.at[2], n)
    summed = added(prk)
    fk[...] = head_norm(summed[:, 0:128], kg[...]).astype(BF16)
    fv[...] = summed[:, 128:256].astype(BF16)

    @pl.when(e != t)
    def _():
        remote(xts, xtr, 3, (t, e)).wait_recv()

    theirs = placed_slots(xtr[:, 256:257], xtr[:, 257:258])
    pt[...] = jnp.transpose(theirs, (1, 0)).astype(BF16)

    lo.wait()
    swaps[3].wait_recv()
    await_blocks(prq, rsem.at[4], n)

    terms[...] = dot(agb[...], wo[...]).astype(BF16)
    for dz in sorted(range(1, deep), key=lambda d: -min(d, deep - d)):
        there = lax.rem(tz + dz, deep)
        remote(terms.at[rows_of(there), :], rsb.at[tz], 5, (e, there * 2 + core)).start()
    rsb[tz] = terms[rows_of(tz), :]
    await_all(rsb.at[pl.ds(0, deep - 1)], rsem.at[5])
    residual = (xtr[:, pl.ds(0, 256)] + added(rsb)).astype(BF16)
    res_s[...] = residual

    picked = dot(pt[...], residual)
    half = (iota((8 * n, 128), 0) // 4) % 2
    disp[...] = (
        jnp.where(half == 0, picked[:, 0:128], picked[:, 128:256]).reshape(n, 8, 128).astype(BF16)
    )

    far = sorted(range(1, deep), key=lambda d: -min(d, deep - d))
    for step in plane_steps(n) + [(0, 0)]:
        p = in_plane(step)
        for dz in far + [0]:
            if dz or step != (0, 0):
                there = lax.rem(tz + dz, deep) * 2 + core
                remote(disp.at[p], xd.at[tz * n + e], 6, (p, there)).start()
    xd[tz * n + e] = disp[e]

    @pl.when(e != t)
    def _():
        remote(res_s, res_r, 7, (t, e)).start()

    @pl.when(e == t)
    def _():
        res_r[...] = res_s[...]

    lg.wait()
    lu.wait()
    experts[0].wait_recv()
    experts[1].wait_recv()

    all_but_one = pl.ds(0, deep * n - 1)
    await_all(xd.at[all_but_one], rsem.at[6])

    arrived = xd[...].reshape(deep, n, 8, 128)
    first = (iota((deep * 8, 128), 0) // 4) % 2 == 0
    squares = jnp.zeros((deep * 8, 128), F32)
    total = jnp.zeros((deep * 8, 512), F32)
    for c in range(n):
        v = arrived[:, c].astype(F32)
        square = v * v
        squares = squares + square.reshape(deep * 8, 128)
        v = (v * geb[c][None]).reshape(deep * 8, 128)
        lhs = jnp.concatenate([jnp.where(first, v, 0.0), jnp.where(first, 0.0, v)], axis=1)
        total = total + dot(lhs.astype(BF16), wgu[pl.ds(c * 256, 256), :])

    def both_halves(v):
        return jnp.concatenate(
            [v[i * 8 : i * 8 + 8] + pltpu.roll(v[i * 8 : i * 8 + 8], 4, 0) for i in range(deep)], axis=0
        )

    squares = jnp.broadcast_to(jnp.sum(squares, axis=1, keepdims=True), (deep * 8, 128))
    scale = lax.rsqrt(both_halves(squares) * (1.0 / width) + EPSILON)
    total = both_halves(total)
    hidden = []
    for k in range(2):
        gate = total[:, k * 256 : k * 256 + 128] * scale
        upward = total[:, k * 256 + 128 : k * 256 + 256] * scale
        hidden.append(gate * jax.nn.sigmoid(gate) * upward)
    hidden = jnp.concatenate(hidden, axis=1).astype(BF16)
    ld.wait()
    experts[2].wait_recv()
    down = dwp[...].reshape(256, width)
    for c in range(n):
        y = dot(hidden, down[:, c * 256 : c * 256 + 256])
        y = jnp.where(first, y[:, 0:128], y[:, 128:256])
        ys[:, c] = y.reshape(deep, 8, 128).astype(BF16)

    def give_back(dz, dc, skip):
        there = lax.rem(tz + dz, deep) * 2 + lax.rem(core + dc, 2)
        for i in range(deep):
            b = 2 * i + core
            cp = remote(ys.at[i, there], rt.at[tz * n + e], 8, (b, there))
            if not skip:
                cp.start()
                continue

            @pl.when(b != e)
            def _():
                cp.start()

            @pl.when(b == e)
            def _():
                rt[tz * n + e] = ys[i, there]

    def give_far(i, c):
        dz = deep // 2 + (i + 1) // 2 * (2 * lax.rem(i, 2) - 1)
        give_back(dz, 0, False)
        give_back(dz, 1, False)
        return c

    lax.fori_loop(0, deep - 1, give_far, 0)
    give_back(0, 1, False)
    give_back(0, 0, True)

    @pl.when(e != t)
    def _():
        remote(res_s, res_r, 7, (t, e)).wait_recv()

    await_blocks(rt, rsem.at[8], deep * n)
    back = rt[pl.ds(0, n)].astype(F32)
    for k in range(1, deep):
        back = back + rt[pl.ds(k * n, n)].astype(F32)
    mixed = dot(cmb[...], back.reshape(8 * n, 128).astype(BF16))
    mixed = mixed[0 : 2 * ROWS] + mixed[2 * ROWS : 4 * ROWS] + mixed[4 * ROWS :]
    mixed = jnp.concatenate([mixed[:ROWS], mixed[ROWS:]], axis=1)
    out[...] = (res_r[...].astype(F32) + mixed).astype(BF16)

    @pl.when(same)
    def _():
        await_all(xn.at[:, pl.ds(0, (n - 1) * 256)], ssem.at[0])

    await_blocks(prq, ssem.at[1], n)
    await_blocks(prk, ssem.at[2], n)
    await_blocks(prq, ssem.at[4], n)
    await_all(rsb.at[pl.ds(0, deep - 1)], ssem.at[5])
    await_all(xd.at[all_but_one], ssem.at[6])
    await_blocks(rt, ssem.at[8], deep * n)
    for cp in swaps + experts:
        cp.wait_send()

    @pl.when(e != t)
    def _():
        remote(xts, xtr, 3, (t, e)).wait_send()
        remote(res_s, res_r, 7, (t, e)).wait_send()


def emit(a, b, c, a_out, b_out, c_out):
    a_out[...] = a[...]
    b_out[...] = b[...]
    c_out[...] = c[...]


def body(
    hidden_in,
    attn_gain,
    query_weight,
    key_weight,
    value_weight,
    query_gain,
    key_gain,
    head_offset,
    key_cache,
    value_cache,
    lengths,
    out_weight,
    expert_gain,
    routes,
    route_weights,
    gate_weight,
    up_weight,
    down_weight,
):
    n = lax.axis_size("ep")
    width = hidden_in.shape[1]
    cache = key_cache.shape[1]
    vmem = pl.BlockSpec(memory_space=pltpu.VMEM)
    hbm = pl.BlockSpec(memory_space=pltpu.HBM)
    V = pltpu.VMEM
    I32 = jnp.int32
    deep = n // 2
    scratch = [
        V((1, width), F32),
        V((1, 128), F32),
        V((1, 128), F32),
        V((1, 2), F32),
        V((1, ROWS), I32),
        V((width // 128, 128), F32),
        V((2, ROWS), I32),
        V((2, ROWS), F32),
        V((ROWS, width), BF16),
        V((ROWS, width), BF16),
        V((deep * ROWS, 256), BF16),
        V((256, 1024), BF16),
        V((deep * ROWS, 512), BF16),
        V((deep * ROWS, 512), BF16),
        V((n, ROWS, 256), BF16),
        V((n, ROWS, 256), BF16),
        V((ROWS, cache, 128), BF16),
        V((ROWS, cache, 128), BF16),
        V((ROWS, 256), BF16),
        V((deep * ROWS, 512), BF16),
        V((512, 256), BF16),
        V((deep * ROWS, 256), BF16),
        V((deep, ROWS, 256), BF16),
        V((ROWS, 384), F32),
        V((ROWS, 384), F32),
        V((ROWS, 256), BF16),
        V((ROWS, 256), BF16),
        V((n, 8, 128), BF16),
        V((deep * n, 8, 128), BF16),
        V((width, 512), BF16),
        V((2, 128, width), BF16),
        V((deep, n, 8, 128), BF16),
        V((deep * n, 8, 128), BF16),
        V((256, 256), BF16),
        V((8 * n, ROWS), BF16),
        V((6 * ROWS, 8 * n), BF16),
        V((n, 8, 128), F32),
        pltpu.SemaphoreType.DMA((20,)),
        pltpu.SemaphoreType.DMA((9,)),
        pltpu.SemaphoreType.DMA((9,)),
        pltpu.SemaphoreType.DMA((7,)),
        pltpu.SemaphoreType.DMA((7,)),
    ]
    results = (
        jax.ShapeDtypeStruct((ROWS, 256), BF16),
        jax.ShapeDtypeStruct((ROWS, 128), BF16),
        jax.ShapeDtypeStruct((ROWS, 128), BF16),
    )
    made = pl.pallas_call(
        functools.partial(kernel, n),
        out_shape=tuple(V(r.shape, r.dtype) for r in results),
        in_specs=[hbm] * 18,
        out_specs=(vmem, vmem, vmem),
        scratch_shapes=scratch,
        compiler_params=pltpu.CompilerParams(
            collective_id=0, has_side_effects=True, vmem_limit_bytes=60 * 1024 * 1024
        ),
    )(
        hidden_in,
        attn_gain.reshape(1, width),
        query_weight,
        key_weight,
        value_weight,
        query_gain.reshape(1, 128),
        key_gain.reshape(1, 128),
        head_offset.reshape(1, 2),
        key_cache,
        value_cache,
        lengths.reshape(1, ROWS),
        out_weight,
        expert_gain.reshape(width // 128, 128),
        routes.T,
        route_weights.T,
        gate_weight,
        up_weight,
        down_weight,
    )
    return pl.pallas_call(
        emit, out_shape=results, in_specs=[vmem] * 3, out_specs=(vmem, vmem, vmem)
    )(*[pltpu.with_memory_space_constraint(m, pltpu.VMEM) for m in made])


def solution(mesh):
    placed = (
        P("ep", None),
        P(),
        P("ep", "tp"),
        P("ep", "tp"),
        P("ep", "tp"),
        P(),
        P(),
        P("tp"),
        P("ep", None, "tp"),
        P("ep", None, "tp"),
        P("ep"),
        P("tp", "ep"),
        P(),
        P("ep", None),
        P("ep", None),
        P("ep", None, "tp"),
        P("ep", None, "tp"),
        P("ep", "tp", None),
    )
    return jax.shard_map(
        body,
        mesh=mesh,
        in_specs=placed,
        out_specs=(P("ep", "tp"), P("ep", "tp"), P("ep", "tp")),
        check_vma=False,
    )
```

```python
import functools
import math

import jax
import jax.numpy as jnp
from jax import lax
from jax.experimental import pallas as pl
from jax.experimental.pallas import tpu as pltpu
from jax.sharding import PartitionSpec as P

EPSILON = 1e-06
MESH = pl.DeviceIdType.MESH
F32 = jnp.float32
BF16 = jnp.bfloat16
ROWS = 16
CAP = 4


def iota(shape, dim):
    return lax.broadcasted_iota(jnp.int32, shape, dim)


def pieces(v):
    hi = v.astype(BF16)
    rest = v - hi.astype(F32)
    mid = rest.astype(BF16)
    low = (rest - mid.astype(F32)).astype(BF16)
    return hi, mid, low


def dot(a, b):
    return jnp.dot(a, b, preferred_element_type=F32)


def plane_steps(n):
    side = math.isqrt(n)
    steps = [(dy, dx) for dy in range(side) for dx in range(side) if (dy, dx) != (0, 0)]
    return sorted(steps, key=lambda s: -sum(min(d, side - d) for d in s))


def column_steps(n):
    deep = n // 2
    steps = [(dz, dc) for dz in range(deep) for dc in range(2) if (dz, dc) != (0, 0)]
    return sorted(steps, key=lambda s: -min(s[0], deep - s[0]))


def kernel(
    n,
    x_h,
    again_h,
    wq_h,
    wk_h,
    wv_h,
    qg_h,
    kg_h,
    ho_h,
    kc_h,
    vc_h,
    lens_h,
    wo_h,
    eg_h,
    routes_h,
    rw_h,
    gw_h,
    uw_h,
    dw_h,
    out,
    fk,
    fv,
    again,
    qg,
    kg,
    ho,
    lens,
    eg,
    routes,
    rw,
    xv,
    xn,
    xg,
    wqkv,
    partq,
    partk,
    prq,
    prk,
    kc,
    vc,
    att,
    agb,
    wo,
    terms,
    rsb,
    xts,
    xtr,
    res_s,
    res_r,
    disp,
    xd,
    wgu,
    dwp,
    ys,
    rt,
    tri,
    pt,
    cmb,
    geb,
    lsem,
    ssem,
    rsem,
    bsend,
    brecv,
):
    e = lax.axis_index("ep")
    t = lax.axis_index("tp")
    side = math.isqrt(n)
    deep = n // 2
    ey, ex = e // side, lax.rem(e, side)
    tz, core = t // 2, lax.rem(t, 2)
    width = n * 256
    cache = kc.shape[1]

    def in_plane(step):
        return lax.rem(ey + step[0], side) * side + lax.rem(ex + step[1], side)

    shift = lax.rem(core + ex, 2)
    parity_steps = sorted(
        [(dy, m) for dy in range(side) for m in range(side // 2)],
        key=lambda s: (-min(s[0], side - s[0]), -s[1]),
    )

    def of_parity(step):
        return lax.rem(ey + step[0], side) * side + lax.rem(ex + shift + 2 * step[1], side)

    same = lax.rem(e, 2) == core
    unlike = lax.rem(e, 2) != core

    def in_column(step):
        return lax.rem(tz + step[0], deep) * 2 + lax.rem(core + step[1], 2)

    bar = pltpu.get_barrier_semaphore()
    for step in plane_steps(n):
        pl.semaphore_signal(bar, inc=1, device_id=(in_plane(step), t), device_id_type=MESH)
    for step in column_steps(n):
        pl.semaphore_signal(bar, inc=1, device_id=(e, in_column(step)), device_id_type=MESH)

    def load(src, dst, k):
        cp = pltpu.make_async_copy(src, dst, lsem.at[k])
        cp.start()
        return cp

    mine256 = pl.multiple_of(core * 256, 256)
    lx = load(x_h, xv, 0)
    small = [load(a, b, 11 + i) for i, (a, b) in enumerate([(again_h, again), (qg_h, qg), (kg_h, kg), (ho_h, ho), (lens_h, lens), (eg_h, eg), (routes_h, routes), (rw_h, rw)])]
    at_q = wqkv.at[:, pl.ds(mine256, 256)]
    at_k = wqkv.at[:, pl.ds(pl.multiple_of(mine256 + 512, 128), 128)]
    at_v = wqkv.at[:, pl.ds(pl.multiple_of(mine256 + 640, 128), 128)]
    at_o = wo.at[pl.ds(pl.multiple_of(core * 256, 256), 256), :]
    lq = load(wq_h, at_q, 1)
    lk = load(wk_h, at_k, 2)
    lv = load(wv_h, at_v, 3)
    lo = load(wo_h, at_o, 4)
    lkc = load(kc_h, kc, 5)
    lvc = load(vc_h, vc, 6)
    lg = load(gw_h.at[0], wgu.at[:, pl.ds(mine256, 128)], 7)
    lu = load(uw_h.at[0], wgu.at[:, pl.ds(pl.multiple_of(mine256 + 128, 128), 128)], 8)
    ld = load(dw_h.at[0], dwp.at[core], 9)

    def remote(src, dst, k, dev, s=ssem, r=rsem):
        return pltpu.make_async_remote_copy(
            src_ref=src,
            dst_ref=dst,
            send_sem=s.at[k],
            recv_sem=r.at[k],
            device_id=dev,
            device_id_type=MESH,
        )

    def rows_of(p, size=ROWS):
        return pl.ds(pl.multiple_of(p * size, size), size)

    def cols_of(p, size=256):
        return pl.ds(pl.multiple_of(p * size, size), size)

    def await_all(ref, sem):
        pltpu.make_async_copy(ref, ref, sem).wait()

    lx.wait()
    small[0].wait()
    x = xv[...].astype(F32)
    meansq = jnp.sum(x * x, axis=1, keepdims=True) * (1.0 / width)
    xn[...] = (x * lax.rsqrt(meansq + EPSILON) * again[...]).astype(BF16)

    pl.semaphore_wait(bar, 2 * (n - 1))

    keeper = tz * 2 + lax.rem(e, 2)

    @pl.when(same)
    def _():
        for step in plane_steps(n):
            p = in_plane(step)
            remote(xn.at[:, cols_of(p)], xg.at[rows_of(e // 2), :], 0, (p, t)).start()
        xg[rows_of(e // 2), :] = xn[:, cols_of(e)]

    other = (e, tz * 2 + 1 - core)
    swaps = [
        remote(wq_h, at_q, 0, other, bsend, brecv),
        remote(wk_h, at_k, 1, other, bsend, brecv),
        remote(wv_h, at_v, 2, other, bsend, brecv),
        remote(wo_h, at_o, 3, other, bsend, brecv),
    ]
    for cp in swaps:
        cp.start()
    others = pl.ds(0, n - 1)

    for cp in small[1:]:
        cp.wait()
    tri[...] = (iota((256, 256), 0) >= iota((256, 256), 1)).astype(F32).astype(BF16)
    lane = iota((ROWS, 8 * n), 1)
    lower = (iota((ROWS, ROWS), 0) > iota((ROWS, ROWS), 1)).astype(F32).astype(BF16)
    diagonal = iota((ROWS, ROWS), 0) == iota((ROWS, ROWS), 1)

    def column(line):
        return jnp.sum(jnp.where(diagonal, line, 0.0), axis=1, keepdims=True)

    expert = (lane // 8).astype(F32)

    def placed_slots(first, second):
        member = jnp.where((first == expert) | (second == expert), 1.0, 0.0)
        rank = dot(lower, member.astype(BF16))
        return jnp.where(rank == (lane % 4).astype(F32), member, 0.0)

    r0 = column(routes[0:1, :].astype(F32))
    r1 = column(routes[1:2, :].astype(F32))
    slots = placed_slots(r0, r1)
    weighted = slots * jnp.where(r0 == expert, column(rw[0:1, :]), column(rw[1:2, :]))
    first_half = jnp.where((lane // 4) % 2 == 0, weighted, 0.0)
    halves = jnp.concatenate([first_half, weighted - first_half], axis=0)
    c_hi, c_mid, c_low = pieces(halves)
    cmb[pl.ds(0, 2 * ROWS), :] = c_hi
    cmb[pl.ds(2 * ROWS, 2 * ROWS), :] = c_mid
    cmb[pl.ds(4 * ROWS, 2 * ROWS), :] = c_low
    for c in range(n):
        geb[c] = jnp.where(
            iota((8, 128), 0) < 4,
            jnp.broadcast_to(eg[2 * c : 2 * c + 1, :], (8, 128)),
            jnp.broadcast_to(eg[2 * c + 1 : 2 * c + 2, :], (8, 128)),
        )
    xts[:, pl.ds(0, 256)] = xv[:, cols_of(t)].astype(F32)
    lanes = iota((ROWS, 128), 1)
    xts[:, pl.ds(256, 128)] = jnp.where(lanes == 0, r0, jnp.where(lanes == 1, r1, 0.0))

    def await_blocks(ref, sem, count):
        @pl.when(same)
        def _():
            await_all(ref.at[pl.ds(0, count - 1)], sem)

        @pl.when(unlike)
        def _():
            await_all(ref, sem)

    lq.wait()
    swaps[0].wait_recv()

    @pl.when(same)
    def _():
        await_all(xg.at[pl.ds(0, (deep - 1) * ROWS), :], rsem.at[0])

    @pl.when(unlike)
    def _():
        await_all(xg, rsem.at[0])

    def to_owners(part, dst, k):
        for step in parity_steps:
            b = of_parity(step)
            for dc in (1, 0):
                there = lax.rem(core + dc, 2)
                cp = remote(part.at[rows_of(b // 2), cols_of(there)], dst.at[e], k, (b, tz * 2 + there))
                if step != (0, 0) or dc == 1:
                    cp.start()
                    continue

                @pl.when(unlike)
                def _():
                    cp.start()

                @pl.when(same)
                def _():
                    dst[e] = part[rows_of(e // 2), cols_of(core)]

    partq[...] = dot(xg[...], wqkv[:, pl.ds(0, 512)]).astype(BF16)
    to_owners(partq, prq, 1)
    lk.wait()
    lv.wait()
    swaps[1].wait_recv()
    swaps[2].wait_recv()
    partk[...] = dot(xg[...], wqkv[:, pl.ds(512, 512)]).astype(BF16)

    @pl.when(e != t)
    def _():
        remote(xts, xtr, 3, (t, e)).start()

    @pl.when(e == t)
    def _():
        xtr[...] = xts[...]

    def head_norm(raw, gain):
        v = raw.astype(BF16).astype(F32)
        meansq = jnp.sum(v * v, axis=1, keepdims=True) * (1.0 / 128)
        return v * lax.rsqrt(meansq + EPSILON) * gain

    def added(ref):
        total = ref[0].astype(F32)
        for k in range(1, ref.shape[0]):
            total = total + ref[k].astype(F32)
        return total

    await_blocks(prq, rsem.at[1], n)

    experts = [
        remote(gw_h.at[0], wgu.at[:, pl.ds(mine256, 128)], 4, other, bsend, brecv),
        remote(
            uw_h.at[0],
            wgu.at[:, pl.ds(pl.multiple_of(mine256 + 128, 128), 128)],
            5,
            other,
            bsend,
            brecv,
        ),
        remote(dw_h.at[0], dwp.at[core], 6, other, bsend, brecv),
    ]
    for cp in experts:
        cp.start()

    summed = added(prq)
    query = jnp.concatenate(
        [head_norm(summed[:, 0:128], qg[...]), head_norm(summed[:, 128:256], qg[...])], axis=0
    )
    row = iota((2 * ROWS, 128), 0)
    lkc.wait()
    z = jnp.zeros((2 * ROWS, cache), F32)
    for b in range(ROWS):
        own = jnp.where(row % ROWS == b, query, 0.0).astype(BF16)
        z = z + lax.dot_general(own, kc[b], (((1,), (1,)), ((), ())), preferred_element_type=F32)
    offset = jnp.where(iota((2 * ROWS, 1), 0) < ROWS, ho[0:1, 0:1], ho[0:1, 1:2])
    z = z * 128**-0.5 + offset
    lens_col = jnp.sum(
        jnp.where(
            iota((2 * ROWS, ROWS), 0) % ROWS == iota((2 * ROWS, ROWS), 1), lens[...].astype(F32), 0.0
        ),
        axis=1,
        keepdims=True,
    )
    live = iota((2 * ROWS, cache), 1).astype(F32) < lens_col
    breaks = jnp.where(live, jnp.maximum(z, 0.0) + jnp.log1p(jnp.exp(-jnp.abs(z))), 0.0)
    chunks = cache // 256
    parts = pieces(breaks)
    stacked = jnp.concatenate(
        [p[:, c * 256 : (c + 1) * 256] for p in parts for c in range(chunks)], axis=0
    )
    sums = dot(stacked, tri[...])
    size = chunks * 2 * ROWS
    sums = sums[:size] + sums[size : 2 * size] + sums[2 * size :]
    after = jnp.zeros((2 * ROWS, 1), F32)
    suffix = [None] * chunks
    for c in range(chunks - 1, -1, -1):
        here = sums[c * 2 * ROWS : (c + 1) * 2 * ROWS]
        suffix[c] = here + after
        after = after + here[:, 0:1]
    suffix = jnp.concatenate(suffix, axis=1)
    stick = jnp.where(live, jnp.exp(z - suffix), 0.0)
    lvc.wait()
    wide_row = iota((2 * ROWS, cache), 0)
    attended = jnp.zeros((2 * ROWS, 128), F32)
    for b in range(ROWS):
        own = jnp.where(wide_row % ROWS == b, stick, 0.0).astype(BF16)
        attended = attended + dot(own, vc[b])
    att[:, pl.ds(0, 128)] = attended[:ROWS].astype(BF16)
    att[:, pl.ds(128, 128)] = attended[ROWS:].astype(BF16)

    heads = agb.at[rows_of(e // 2), cols_of(core)]
    for step in plane_steps(n):
        remote(att, heads, 4, (in_plane(step), keeper)).start()

    @pl.when(unlike)
    def _():
        remote(att, heads, 4, other).start()

    @pl.when(same)
    def _():
        agb[rows_of(e // 2), cols_of(core)] = att[...]

    @pl.when(e != t)
    def _():
        remote(xts, xtr, 3, (t, e)).wait_recv()

    theirs = placed_slots(xtr[:, 256:257], xtr[:, 257:258])
    pt[...] = jnp.transpose(theirs, (1, 0)).astype(BF16)

    lo.wait()
    swaps[3].wait_recv()
    await_blocks(prq, rsem.at[4], n)

    terms[...] = dot(agb[...], wo[...]).astype(BF16)
    for dz in sorted(range(1, deep), key=lambda d: -min(d, deep - d)):
        there = lax.rem(tz + dz, deep)
        remote(terms.at[rows_of(there), :], rsb.at[tz], 5, (e, there * 2 + core)).start()
    rsb[tz] = terms[rows_of(tz), :]

    to_owners(partk, prk, 2)
    await_all(rsb.at[pl.ds(0, deep - 1)], rsem.at[5])
    residual = (xtr[:, pl.ds(0, 256)] + added(rsb)).astype(BF16)
    res_s[...] = residual

    picked = dot(pt[...], residual)
    half = (iota((8 * n, 128), 0) // 4) % 2
    disp[...] = (
        jnp.where(half == 0, picked[:, 0:128], picked[:, 128:256]).reshape(n, 8, 128).astype(BF16)
    )

    far = sorted(range(1, deep), key=lambda d: -min(d, deep - d))
    for step in plane_steps(n) + [(0, 0)]:
        p = in_plane(step)
        for dz in far + [0]:
            if dz or step != (0, 0):
                there = lax.rem(tz + dz, deep) * 2 + core
                remote(disp.at[p], xd.at[tz * n + e], 6, (p, there)).start()
    xd[tz * n + e] = disp[e]

    @pl.when(e != t)
    def _():
        remote(res_s, res_r, 7, (t, e)).start()

    @pl.when(e == t)
    def _():
        res_r[...] = res_s[...]

    lg.wait()
    lu.wait()
    experts[0].wait_recv()
    experts[1].wait_recv()

    all_but_one = pl.ds(0, deep * n - 1)
    await_all(xd.at[all_but_one], rsem.at[6])

    arrived = xd[...].reshape(deep, n, 8, 128)
    first = (iota((deep * 8, 128), 0) // 4) % 2 == 0
    squares = jnp.zeros((deep * 8, 128), F32)
    total = jnp.zeros((deep * 8, 512), F32)
    for c in range(n):
        v = arrived[:, c].astype(F32)
        square = v * v
        squares = squares + square.reshape(deep * 8, 128)
        v = (v * geb[c][None]).reshape(deep * 8, 128)
        lhs = jnp.concatenate([jnp.where(first, v, 0.0), jnp.where(first, 0.0, v)], axis=1)
        total = total + dot(lhs.astype(BF16), wgu[pl.ds(c * 256, 256), :])

    def both_halves(v):
        return jnp.concatenate(
            [v[i * 8 : i * 8 + 8] + pltpu.roll(v[i * 8 : i * 8 + 8], 4, 0) for i in range(deep)], axis=0
        )

    squares = jnp.broadcast_to(jnp.sum(squares, axis=1, keepdims=True), (deep * 8, 128))
    scale = lax.rsqrt(both_halves(squares) * (1.0 / width) + EPSILON)
    total = both_halves(total)
    hidden = []
    for k in range(2):
        gate = total[:, k * 256 : k * 256 + 128] * scale
        upward = total[:, k * 256 + 128 : k * 256 + 256] * scale
        hidden.append(gate * jax.nn.sigmoid(gate) * upward)
    hidden = jnp.concatenate(hidden, axis=1).astype(BF16)
    ld.wait()
    experts[2].wait_recv()
    down = dwp[...].reshape(256, width)
    for c in range(n):
        y = dot(hidden, down[:, c * 256 : c * 256 + 256])
        y = jnp.where(first, y[:, 0:128], y[:, 128:256])
        ys[:, c] = y.reshape(deep, 8, 128).astype(BF16)

    def give_back(dz, dc, skip):
        there = lax.rem(tz + dz, deep) * 2 + lax.rem(core + dc, 2)
        for i in range(deep):
            b = 2 * i + core
            cp = remote(ys.at[i, there], rt.at[tz * n + e], 8, (b, there))
            if not skip:
                cp.start()
                continue

            @pl.when(b != e)
            def _():
                cp.start()

            @pl.when(b == e)
            def _():
                rt[tz * n + e] = ys[i, there]

    def give_far(i, c):
        dz = deep // 2 + (i + 1) // 2 * (2 * lax.rem(i, 2) - 1)
        give_back(dz, 0, False)
        give_back(dz, 1, False)
        return c

    lax.fori_loop(0, deep - 1, give_far, 0)
    give_back(0, 1, False)
    give_back(0, 0, True)

    await_blocks(prk, rsem.at[2], n)
    summed = added(prk)
    fk[...] = head_norm(summed[:, 0:128], kg[...]).astype(BF16)
    fv[...] = summed[:, 128:256].astype(BF16)

    @pl.when(e != t)
    def _():
        remote(res_s, res_r, 7, (t, e)).wait_recv()

    await_blocks(rt, rsem.at[8], deep * n)
    back = rt[pl.ds(0, n)].astype(F32)
    for k in range(1, deep):
        back = back + rt[pl.ds(k * n, n)].astype(F32)
    mixed = dot(cmb[...], back.reshape(8 * n, 128).astype(BF16))
    mixed = mixed[0 : 2 * ROWS] + mixed[2 * ROWS : 4 * ROWS] + mixed[4 * ROWS :]
    mixed = jnp.concatenate([mixed[:ROWS], mixed[ROWS:]], axis=1)
    out[...] = (res_r[...].astype(F32) + mixed).astype(BF16)

    @pl.when(same)
    def _():
        await_all(xn.at[:, pl.ds(0, (n - 1) * 256)], ssem.at[0])

    await_blocks(prq, ssem.at[1], n)
    await_blocks(prk, ssem.at[2], n)
    await_blocks(prq, ssem.at[4], n)
    await_all(rsb.at[pl.ds(0, deep - 1)], ssem.at[5])
    await_all(xd.at[all_but_one], ssem.at[6])
    await_blocks(rt, ssem.at[8], deep * n)
    for cp in swaps + experts:
        cp.wait_send()

    @pl.when(e != t)
    def _():
        remote(xts, xtr, 3, (t, e)).wait_send()
        remote(res_s, res_r, 7, (t, e)).wait_send()


def emit(a, b, c, a_out, b_out, c_out):
    a_out[...] = a[...]
    b_out[...] = b[...]
    c_out[...] = c[...]


def body(
    hidden_in,
    attn_gain,
    query_weight,
    key_weight,
    value_weight,
    query_gain,
    key_gain,
    head_offset,
    key_cache,
    value_cache,
    lengths,
    out_weight,
    expert_gain,
    routes,
    route_weights,
    gate_weight,
    up_weight,
    down_weight,
):
    n = lax.axis_size("ep")
    width = hidden_in.shape[1]
    cache = key_cache.shape[1]
    vmem = pl.BlockSpec(memory_space=pltpu.VMEM)
    hbm = pl.BlockSpec(memory_space=pltpu.HBM)
    V = pltpu.VMEM
    I32 = jnp.int32
    deep = n // 2
    scratch = [
        V((1, width), F32),
        V((1, 128), F32),
        V((1, 128), F32),
        V((1, 2), F32),
        V((1, ROWS), I32),
        V((width // 128, 128), F32),
        V((2, ROWS), I32),
        V((2, ROWS), F32),
        V((ROWS, width), BF16),
        V((ROWS, width), BF16),
        V((deep * ROWS, 256), BF16),
        V((256, 1024), BF16),
        V((deep * ROWS, 512), BF16),
        V((deep * ROWS, 512), BF16),
        V((n, ROWS, 256), BF16),
        V((n, ROWS, 256), BF16),
        V((ROWS, cache, 128), BF16),
        V((ROWS, cache, 128), BF16),
        V((ROWS, 256), BF16),
        V((deep * ROWS, 512), BF16),
        V((512, 256), BF16),
        V((deep * ROWS, 256), BF16),
        V((deep, ROWS, 256), BF16),
        V((ROWS, 384), F32),
        V((ROWS, 384), F32),
        V((ROWS, 256), BF16),
        V((ROWS, 256), BF16),
        V((n, 8, 128), BF16),
        V((deep * n, 8, 128), BF16),
        V((width, 512), BF16),
        V((2, 128, width), BF16),
        V((deep, n, 8, 128), BF16),
        V((deep * n, 8, 128), BF16),
        V((256, 256), BF16),
        V((8 * n, ROWS), BF16),
        V((6 * ROWS, 8 * n), BF16),
        V((n, 8, 128), F32),
        pltpu.SemaphoreType.DMA((20,)),
        pltpu.SemaphoreType.DMA((9,)),
        pltpu.SemaphoreType.DMA((9,)),
        pltpu.SemaphoreType.DMA((7,)),
        pltpu.SemaphoreType.DMA((7,)),
    ]
    results = (
        jax.ShapeDtypeStruct((ROWS, 256), BF16),
        jax.ShapeDtypeStruct((ROWS, 128), BF16),
        jax.ShapeDtypeStruct((ROWS, 128), BF16),
    )
    made = pl.pallas_call(
        functools.partial(kernel, n),
        out_shape=tuple(V(r.shape, r.dtype) for r in results),
        in_specs=[hbm] * 18,
        out_specs=(vmem, vmem, vmem),
        scratch_shapes=scratch,
        compiler_params=pltpu.CompilerParams(
            collective_id=0, has_side_effects=True, vmem_limit_bytes=60 * 1024 * 1024
        ),
    )(
        hidden_in,
        attn_gain.reshape(1, width),
        query_weight,
        key_weight,
        value_weight,
        query_gain.reshape(1, 128),
        key_gain.reshape(1, 128),
        head_offset.reshape(1, 2),
        key_cache,
        value_cache,
        lengths.reshape(1, ROWS),
        out_weight,
        expert_gain.reshape(width // 128, 128),
        routes.T,
        route_weights.T,
        gate_weight,
        up_weight,
        down_weight,
    )
    return pl.pallas_call(
        emit, out_shape=results, in_specs=[vmem] * 3, out_specs=(vmem, vmem, vmem)
    )(*[pltpu.with_memory_space_constraint(m, pltpu.VMEM) for m in made])


def solution(mesh):
    placed = (
        P("ep", None),
        P(),
        P("ep", "tp"),
        P("ep", "tp"),
        P("ep", "tp"),
        P(),
        P(),
        P("tp"),
        P("ep", None, "tp"),
        P("ep", None, "tp"),
        P("ep"),
        P("tp", "ep"),
        P(),
        P("ep", None),
        P("ep", None),
        P("ep", None, "tp"),
        P("ep", None, "tp"),
        P("ep", "tp", None),
    )
    return jax.shard_map(
        body,
        mesh=mesh,
        in_specs=placed,
        out_specs=(P("ep", "tp"), P("ep", "tp"), P("ep", "tp")),
        check_vma=False,
    )
```

```python
import functools
import math

import jax
import jax.numpy as jnp
from jax import lax
from jax.experimental import pallas as pl
from jax.experimental.pallas import tpu as pltpu
from jax.sharding import PartitionSpec as P

EPSILON = 1e-06
MESH = pl.DeviceIdType.MESH
F32 = jnp.float32
BF16 = jnp.bfloat16
ROWS = 16
CAP = 4


def iota(shape, dim):
    return lax.broadcasted_iota(jnp.int32, shape, dim)


def pieces(v):
    hi = v.astype(BF16)
    rest = v - hi.astype(F32)
    mid = rest.astype(BF16)
    low = (rest - mid.astype(F32)).astype(BF16)
    return hi, mid, low


def dot(a, b):
    return jnp.dot(a, b, preferred_element_type=F32)


def plane_steps(n):
    side = math.isqrt(n)
    steps = [(dy, dx) for dy in range(side) for dx in range(side) if (dy, dx) != (0, 0)]
    return sorted(steps, key=lambda s: -sum(min(d, side - d) for d in s))


def column_steps(n):
    deep = n // 2
    steps = [(dz, dc) for dz in range(deep) for dc in range(2) if (dz, dc) != (0, 0)]
    return sorted(steps, key=lambda s: -min(s[0], deep - s[0]))


def kernel(
    n,
    x_h,
    again_h,
    wq_h,
    wk_h,
    wv_h,
    qg_h,
    kg_h,
    ho_h,
    kc_h,
    vc_h,
    lens_h,
    wo_h,
    eg_h,
    routes_h,
    rw_h,
    gw_h,
    uw_h,
    dw_h,
    out,
    fk,
    fv,
    again,
    qg,
    kg,
    ho,
    lens,
    eg,
    routes,
    rw,
    xv,
    xn,
    xg,
    wqkv,
    partq,
    partk,
    prq,
    prk,
    kc,
    vc,
    att,
    agb,
    wo,
    terms,
    rsb,
    xts,
    xtr,
    res_s,
    res_r,
    disp,
    xd,
    wgu,
    dwp,
    ys,
    rt,
    tri,
    pt,
    cmb,
    geb,
    lsem,
    ssem,
    rsem,
    bsend,
    brecv,
):
    e = lax.axis_index("ep")
    t = lax.axis_index("tp")
    side = math.isqrt(n)
    deep = n // 2
    ey, ex = e // side, lax.rem(e, side)
    tz, core = t // 2, lax.rem(t, 2)
    width = n * 256
    cache = kc.shape[1]

    def in_plane(step):
        return lax.rem(ey + step[0], side) * side + lax.rem(ex + step[1], side)

    shift = lax.rem(core + ex, 2)
    parity_steps = sorted(
        [(dy, m) for dy in range(side) for m in range(side // 2)],
        key=lambda s: (-min(s[0], side - s[0]), -s[1]),
    )

    def of_parity(step):
        return lax.rem(ey + step[0], side) * side + lax.rem(ex + shift + 2 * step[1], side)

    same = lax.rem(e, 2) == core
    unlike = lax.rem(e, 2) != core

    def in_column(step):
        return lax.rem(tz + step[0], deep) * 2 + lax.rem(core + step[1], 2)

    bar = pltpu.get_barrier_semaphore()
    for step in plane_steps(n):
        pl.semaphore_signal(bar, inc=1, device_id=(in_plane(step), t), device_id_type=MESH)
    for step in column_steps(n):
        pl.semaphore_signal(bar, inc=1, device_id=(e, in_column(step)), device_id_type=MESH)

    def load(src, dst, k):
        cp = pltpu.make_async_copy(src, dst, lsem.at[k])
        cp.start()
        return cp

    mine256 = pl.multiple_of(core * 256, 256)
    lx = load(x_h, xv, 0)
    small = [load(a, b, 11 + i) for i, (a, b) in enumerate([(again_h, again), (qg_h, qg), (kg_h, kg), (ho_h, ho), (lens_h, lens), (eg_h, eg), (routes_h, routes), (rw_h, rw)])]
    at_q = wqkv.at[:, pl.ds(mine256, 256)]
    at_k = wqkv.at[:, pl.ds(pl.multiple_of(mine256 + 512, 128), 128)]
    at_v = wqkv.at[:, pl.ds(pl.multiple_of(mine256 + 640, 128), 128)]
    at_o = wo.at[pl.ds(pl.multiple_of(core * 256, 256), 256), :]
    lq = load(wq_h, at_q, 1)
    lk = load(wk_h, at_k, 2)
    lv = load(wv_h, at_v, 3)
    lo = load(wo_h, at_o, 4)
    lkc = load(kc_h, kc, 5)
    lvc = load(vc_h, vc, 6)
    lg = load(gw_h.at[0], wgu.at[:, pl.ds(mine256, 128)], 7)
    lu = load(uw_h.at[0], wgu.at[:, pl.ds(pl.multiple_of(mine256 + 128, 128), 128)], 8)
    ld = load(dw_h.at[0], dwp.at[core], 9)

    def remote(src, dst, k, dev, s=ssem, r=rsem):
        return pltpu.make_async_remote_copy(
            src_ref=src,
            dst_ref=dst,
            send_sem=s.at[k],
            recv_sem=r.at[k],
            device_id=dev,
            device_id_type=MESH,
        )

    def rows_of(p, size=ROWS):
        return pl.ds(pl.multiple_of(p * size, size), size)

    def cols_of(p, size=256):
        return pl.ds(pl.multiple_of(p * size, size), size)

    def await_all(ref, sem):
        pltpu.make_async_copy(ref, ref, sem).wait()

    lx.wait()
    small[0].wait()
    x = xv[...].astype(F32)
    meansq = jnp.sum(x * x, axis=1, keepdims=True) * (1.0 / width)
    xn[...] = (x * lax.rsqrt(meansq + EPSILON) * again[...]).astype(BF16)

    pl.semaphore_wait(bar, 2 * (n - 1))

    keeper = tz * 2 + lax.rem(e, 2)

    @pl.when(same)
    def _():
        for step in plane_steps(n):
            p = in_plane(step)
            remote(xn.at[:, cols_of(p)], xg.at[rows_of(e // 2), :], 0, (p, t)).start()
        xg[rows_of(e // 2), :] = xn[:, cols_of(e)]

    other = (e, tz * 2 + 1 - core)
    swaps = [
        remote(wq_h, at_q, 0, other, bsend, brecv),
        remote(wk_h, at_k, 1, other, bsend, brecv),
        remote(wv_h, at_v, 2, other, bsend, brecv),
        remote(wo_h, at_o, 3, other, bsend, brecv),
    ]
    for cp in swaps:
        cp.start()
    others = pl.ds(0, n - 1)

    for cp in small[1:]:
        cp.wait()
    tri[...] = (iota((256, 256), 0) >= iota((256, 256), 1)).astype(F32).astype(BF16)
    lane = iota((ROWS, 8 * n), 1)
    lower = (iota((ROWS, ROWS), 0) > iota((ROWS, ROWS), 1)).astype(F32).astype(BF16)
    diagonal = iota((ROWS, ROWS), 0) == iota((ROWS, ROWS), 1)

    def column(line):
        return jnp.sum(jnp.where(diagonal, line, 0.0), axis=1, keepdims=True)

    expert = (lane // 8).astype(F32)

    def placed_slots(first, second):
        member = jnp.where((first == expert) | (second == expert), 1.0, 0.0)
        rank = dot(lower, member.astype(BF16))
        return jnp.where(rank == (lane % 4).astype(F32), member, 0.0)

    r0 = column(routes[0:1, :].astype(F32))
    r1 = column(routes[1:2, :].astype(F32))
    slots = placed_slots(r0, r1)
    weighted = slots * jnp.where(r0 == expert, column(rw[0:1, :]), column(rw[1:2, :]))
    first_half = jnp.where((lane // 4) % 2 == 0, weighted, 0.0)
    halves = jnp.concatenate([first_half, weighted - first_half], axis=0)
    c_hi, c_mid, c_low = pieces(halves)
    cmb[pl.ds(0, 2 * ROWS), :] = c_hi
    cmb[pl.ds(2 * ROWS, 2 * ROWS), :] = c_mid
    cmb[pl.ds(4 * ROWS, 2 * ROWS), :] = c_low
    for c in range(n):
        geb[c] = jnp.where(
            iota((8, 128), 0) < 4,
            jnp.broadcast_to(eg[2 * c : 2 * c + 1, :], (8, 128)),
            jnp.broadcast_to(eg[2 * c + 1 : 2 * c + 2, :], (8, 128)),
        )
    xts[:, pl.ds(0, 256)] = xv[:, cols_of(t)].astype(F32)
    lanes = iota((ROWS, 128), 1)
    xts[:, pl.ds(256, 128)] = jnp.where(lanes == 0, r0, jnp.where(lanes == 1, r1, 0.0))

    def await_blocks(ref, sem, count):
        @pl.when(same)
        def _():
            await_all(ref.at[pl.ds(0, count - 1)], sem)

        @pl.when(unlike)
        def _():
            await_all(ref, sem)

    lq.wait()
    swaps[0].wait_recv()

    @pl.when(same)
    def _():
        await_all(xg.at[pl.ds(0, (deep - 1) * ROWS), :], rsem.at[0])

    @pl.when(unlike)
    def _():
        await_all(xg, rsem.at[0])

    def to_owners(part, dst, k):
        for step in parity_steps:
            b = of_parity(step)
            for dc in (1, 0):
                there = lax.rem(core + dc, 2)
                cp = remote(part.at[rows_of(b // 2), cols_of(there)], dst.at[e], k, (b, tz * 2 + there))
                if step != (0, 0) or dc == 1:
                    cp.start()
                    continue

                @pl.when(unlike)
                def _():
                    cp.start()

                @pl.when(same)
                def _():
                    dst[e] = part[rows_of(e // 2), cols_of(core)]

    partq[...] = dot(xg[...], wqkv[:, pl.ds(0, 512)]).astype(BF16)
    to_owners(partq, prq, 1)
    lk.wait()
    lv.wait()
    swaps[1].wait_recv()
    swaps[2].wait_recv()
    partk[...] = dot(xg[...], wqkv[:, pl.ds(512, 512)]).astype(BF16)

    @pl.when(e != t)
    def _():
        remote(xts, xtr, 3, (t, e)).start()

    @pl.when(e == t)
    def _():
        xtr[...] = xts[...]

    def head_norm(raw, gain):
        v = raw.astype(BF16).astype(F32)
        meansq = jnp.sum(v * v, axis=1, keepdims=True) * (1.0 / 128)
        return v * lax.rsqrt(meansq + EPSILON) * gain

    def added(ref):
        total = ref[0].astype(F32)
        for k in range(1, ref.shape[0]):
            total = total + ref[k].astype(F32)
        return total

    await_blocks(prq, rsem.at[1], n)

    experts = [
        remote(gw_h.at[0], wgu.at[:, pl.ds(mine256, 128)], 4, other, bsend, brecv),
        remote(
            uw_h.at[0],
            wgu.at[:, pl.ds(pl.multiple_of(mine256 + 128, 128), 128)],
            5,
            other,
            bsend,
            brecv,
        ),
        remote(dw_h.at[0], dwp.at[core], 6, other, bsend, brecv),
    ]
    for cp in experts:
        cp.start()

    summed = added(prq)
    query = jnp.concatenate(
        [head_norm(summed[:, 0:128], qg[...]), head_norm(summed[:, 128:256], qg[...])], axis=0
    )
    row = iota((2 * ROWS, 128), 0)
    lkc.wait()
    z = jnp.zeros((2 * ROWS, cache), F32)
    for b in range(ROWS):
        own = jnp.where(row % ROWS == b, query, 0.0).astype(BF16)
        z = z + lax.dot_general(own, kc[b], (((1,), (1,)), ((), ())), preferred_element_type=F32)
    offset = jnp.where(iota((2 * ROWS, 1), 0) < ROWS, ho[0:1, 0:1], ho[0:1, 1:2])
    z = z * 128**-0.5 + offset
    lens_col = jnp.sum(
        jnp.where(
            iota((2 * ROWS, ROWS), 0) % ROWS == iota((2 * ROWS, ROWS), 1), lens[...].astype(F32), 0.0
        ),
        axis=1,
        keepdims=True,
    )
    live = iota((2 * ROWS, cache), 1).astype(F32) < lens_col
    breaks = jnp.where(live, jnp.maximum(z, 0.0) + jnp.log1p(jnp.exp(-jnp.abs(z))), 0.0)
    chunks = cache // 256
    parts = pieces(breaks)
    stacked = jnp.concatenate(
        [p[:, c * 256 : (c + 1) * 256] for p in parts for c in range(chunks)], axis=0
    )
    sums = dot(stacked, tri[...])
    size = chunks * 2 * ROWS
    sums = sums[:size] + sums[size : 2 * size] + sums[2 * size :]
    after = jnp.zeros((2 * ROWS, 1), F32)
    suffix = [None] * chunks
    for c in range(chunks - 1, -1, -1):
        here = sums[c * 2 * ROWS : (c + 1) * 2 * ROWS]
        suffix[c] = here + after
        after = after + here[:, 0:1]
    suffix = jnp.concatenate(suffix, axis=1)
    stick = jnp.where(live, jnp.exp(z - suffix), 0.0)
    lvc.wait()
    wide_row = iota((2 * ROWS, cache), 0)
    attended = jnp.zeros((2 * ROWS, 128), F32)
    for b in range(ROWS):
        own = jnp.where(wide_row % ROWS == b, stick, 0.0).astype(BF16)
        attended = attended + dot(own, vc[b])
    att[:, pl.ds(0, 128)] = attended[:ROWS].astype(BF16)
    att[:, pl.ds(128, 128)] = attended[ROWS:].astype(BF16)

    heads = agb.at[rows_of(e // 2), cols_of(core)]
    for step in plane_steps(n):
        remote(att, heads, 4, (in_plane(step), keeper)).start()

    @pl.when(unlike)
    def _():
        remote(att, heads, 4, other).start()

    @pl.when(same)
    def _():
        agb[rows_of(e // 2), cols_of(core)] = att[...]

    @pl.when(e != t)
    def _():
        remote(xts, xtr, 3, (t, e)).wait_recv()

    theirs = placed_slots(xtr[:, 256:257], xtr[:, 257:258])
    pt[...] = jnp.transpose(theirs, (1, 0)).astype(BF16)

    lo.wait()
    swaps[3].wait_recv()
    await_blocks(prq, rsem.at[4], n)

    terms[...] = dot(agb[...], wo[...]).astype(BF16)
    for dz in sorted(range(1, deep), key=lambda d: -min(d, deep - d)):
        there = lax.rem(tz + dz, deep)
        remote(terms.at[rows_of(there), :], rsb.at[tz], 5, (e, there * 2 + core)).start()
    rsb[tz] = terms[rows_of(tz), :]

    to_owners(partk, prk, 2)
    await_all(rsb.at[pl.ds(0, deep - 1)], rsem.at[5])
    residual = (xtr[:, pl.ds(0, 256)] + added(rsb)).astype(BF16)
    res_s[...] = residual

    picked = dot(pt[...], residual)
    half = (iota((8 * n, 128), 0) // 4) % 2
    disp[...] = (
        jnp.where(half == 0, picked[:, 0:128], picked[:, 128:256]).reshape(n, 8, 128).astype(BF16)
    )

    far = sorted(range(1, deep), key=lambda d: -min(d, deep - d))
    for step in plane_steps(n) + [(0, 0)]:
        p = in_plane(step)
        for dz in far + [0]:
            if dz or step != (0, 0):
                there = lax.rem(tz + dz, deep) * 2 + core
                remote(disp.at[p], xd.at[tz * n + e], 6, (p, there)).start()
    xd[tz * n + e] = disp[e]

    @pl.when(e != t)
    def _():
        remote(res_s, res_r, 7, (t, e)).start()

    @pl.when(e == t)
    def _():
        res_r[...] = res_s[...]

    lg.wait()
    lu.wait()
    experts[0].wait_recv()
    experts[1].wait_recv()

    all_but_one = pl.ds(0, deep * n - 1)
    await_all(xd.at[all_but_one], rsem.at[6])

    arrived = xd[...].reshape(deep, n, 8, 128)
    first = (iota((deep * 8, 128), 0) // 4) % 2 == 0
    squares = jnp.zeros((deep * 8, 128), F32)
    total = jnp.zeros((deep * 8, 512), F32)
    for c in range(n):
        v = arrived[:, c].astype(F32)
        square = v * v
        squares = squares + square.reshape(deep * 8, 128)
        v = (v * geb[c][None]).reshape(deep * 8, 128)
        lhs = jnp.concatenate([jnp.where(first, v, 0.0), jnp.where(first, 0.0, v)], axis=1)
        total = total + dot(lhs.astype(BF16), wgu[pl.ds(c * 256, 256), :])

    def both_halves(v):
        return jnp.concatenate(
            [v[i * 8 : i * 8 + 8] + pltpu.roll(v[i * 8 : i * 8 + 8], 4, 0) for i in range(deep)], axis=0
        )

    squares = jnp.broadcast_to(jnp.sum(squares, axis=1, keepdims=True), (deep * 8, 128))
    scale = lax.rsqrt(both_halves(squares) * (1.0 / width) + EPSILON)
    total = both_halves(total)
    hidden = []
    for k in range(2):
        gate = total[:, k * 256 : k * 256 + 128] * scale
        upward = total[:, k * 256 + 128 : k * 256 + 256] * scale
        hidden.append(gate * jax.nn.sigmoid(gate) * upward)
    hidden = jnp.concatenate(hidden, axis=1).astype(BF16)
    ld.wait()
    experts[2].wait_recv()
    down = dwp[...].reshape(256, width)
    for c in range(n):
        y = dot(hidden, down[:, c * 256 : c * 256 + 256])
        y = jnp.where(first, y[:, 0:128], y[:, 128:256])
        ys[:, c] = y.reshape(deep, 8, 128).astype(BF16)

    for step in parity_steps:
        b = of_parity(step)
        for dz in far + [0]:
            for dc in (0, 1) if dz else (1, 0):
                there = lax.rem(tz + dz, deep) * 2 + lax.rem(core + dc, 2)
                cp = remote(ys.at[b // 2, there], rt.at[tz * n + e], 8, (b, there))
                if step != (0, 0) or dz or dc:
                    cp.start()
                    continue

                @pl.when(unlike)
                def _():
                    cp.start()

                @pl.when(same)
                def _():
                    rt[tz * n + e] = ys[e // 2, t]

    await_blocks(prk, rsem.at[2], n)
    summed = added(prk)
    fk[...] = head_norm(summed[:, 0:128], kg[...]).astype(BF16)
    fv[...] = summed[:, 128:256].astype(BF16)

    @pl.when(e != t)
    def _():
        remote(res_s, res_r, 7, (t, e)).wait_recv()

    await_blocks(rt, rsem.at[8], deep * n)
    back = rt[pl.ds(0, n)].astype(F32)
    for k in range(1, deep):
        back = back + rt[pl.ds(k * n, n)].astype(F32)
    mixed = dot(cmb[...], back.reshape(8 * n, 128).astype(BF16))
    mixed = mixed[0 : 2 * ROWS] + mixed[2 * ROWS : 4 * ROWS] + mixed[4 * ROWS :]
    mixed = jnp.concatenate([mixed[:ROWS], mixed[ROWS:]], axis=1)
    out[...] = (res_r[...].astype(F32) + mixed).astype(BF16)

    @pl.when(same)
    def _():
        await_all(xn.at[:, pl.ds(0, (n - 1) * 256)], ssem.at[0])

    await_blocks(prq, ssem.at[1], n)
    await_blocks(prk, ssem.at[2], n)
    await_blocks(prq, ssem.at[4], n)
    await_all(rsb.at[pl.ds(0, deep - 1)], ssem.at[5])
    await_all(xd.at[all_but_one], ssem.at[6])
    await_blocks(rt, ssem.at[8], deep * n)
    for cp in swaps + experts:
        cp.wait_send()

    @pl.when(e != t)
    def _():
        remote(xts, xtr, 3, (t, e)).wait_send()
        remote(res_s, res_r, 7, (t, e)).wait_send()


def emit(a, b, c, a_out, b_out, c_out):
    a_out[...] = a[...]
    b_out[...] = b[...]
    c_out[...] = c[...]


def body(
    hidden_in,
    attn_gain,
    query_weight,
    key_weight,
    value_weight,
    query_gain,
    key_gain,
    head_offset,
    key_cache,
    value_cache,
    lengths,
    out_weight,
    expert_gain,
    routes,
    route_weights,
    gate_weight,
    up_weight,
    down_weight,
):
    n = lax.axis_size("ep")
    width = hidden_in.shape[1]
    cache = key_cache.shape[1]
    vmem = pl.BlockSpec(memory_space=pltpu.VMEM)
    hbm = pl.BlockSpec(memory_space=pltpu.HBM)
    V = pltpu.VMEM
    I32 = jnp.int32
    deep = n // 2
    scratch = [
        V((1, width), F32),
        V((1, 128), F32),
        V((1, 128), F32),
        V((1, 2), F32),
        V((1, ROWS), I32),
        V((width // 128, 128), F32),
        V((2, ROWS), I32),
        V((2, ROWS), F32),
        V((ROWS, width), BF16),
        V((ROWS, width), BF16),
        V((deep * ROWS, 256), BF16),
        V((256, 1024), BF16),
        V((deep * ROWS, 512), BF16),
        V((deep * ROWS, 512), BF16),
        V((n, ROWS, 256), BF16),
        V((n, ROWS, 256), BF16),
        V((ROWS, cache, 128), BF16),
        V((ROWS, cache, 128), BF16),
        V((ROWS, 256), BF16),
        V((deep * ROWS, 512), BF16),
        V((512, 256), BF16),
        V((deep * ROWS, 256), BF16),
        V((deep, ROWS, 256), BF16),
        V((ROWS, 384), F32),
        V((ROWS, 384), F32),
        V((ROWS, 256), BF16),
        V((ROWS, 256), BF16),
        V((n, 8, 128), BF16),
        V((deep * n, 8, 128), BF16),
        V((width, 512), BF16),
        V((2, 128, width), BF16),
        V((deep, n, 8, 128), BF16),
        V((deep * n, 8, 128), BF16),
        V((256, 256), BF16),
        V((8 * n, ROWS), BF16),
        V((6 * ROWS, 8 * n), BF16),
        V((n, 8, 128), F32),
        pltpu.SemaphoreType.DMA((20,)),
        pltpu.SemaphoreType.DMA((9,)),
        pltpu.SemaphoreType.DMA((9,)),
        pltpu.SemaphoreType.DMA((7,)),
        pltpu.SemaphoreType.DMA((7,)),
    ]
    results = (
        jax.ShapeDtypeStruct((ROWS, 256), BF16),
        jax.ShapeDtypeStruct((ROWS, 128), BF16),
        jax.ShapeDtypeStruct((ROWS, 128), BF16),
    )
    made = pl.pallas_call(
        functools.partial(kernel, n),
        out_shape=tuple(V(r.shape, r.dtype) for r in results),
        in_specs=[hbm] * 18,
        out_specs=(vmem, vmem, vmem),
        scratch_shapes=scratch,
        compiler_params=pltpu.CompilerParams(
            collective_id=0, has_side_effects=True, vmem_limit_bytes=60 * 1024 * 1024
        ),
    )(
        hidden_in,
        attn_gain.reshape(1, width),
        query_weight,
        key_weight,
        value_weight,
        query_gain.reshape(1, 128),
        key_gain.reshape(1, 128),
        head_offset.reshape(1, 2),
        key_cache,
        value_cache,
        lengths.reshape(1, ROWS),
        out_weight,
        expert_gain.reshape(width // 128, 128),
        routes.T,
        route_weights.T,
        gate_weight,
        up_weight,
        down_weight,
    )
    return pl.pallas_call(
        emit, out_shape=results, in_specs=[vmem] * 3, out_specs=(vmem, vmem, vmem)
    )(*[pltpu.with_memory_space_constraint(m, pltpu.VMEM) for m in made])


def solution(mesh):
    placed = (
        P("ep", None),
        P(),
        P("ep", "tp"),
        P("ep", "tp"),
        P("ep", "tp"),
        P(),
        P(),
        P("tp"),
        P("ep", None, "tp"),
        P("ep", None, "tp"),
        P("ep"),
        P("tp", "ep"),
        P(),
        P("ep", None),
        P("ep", None),
        P("ep", None, "tp"),
        P("ep", None, "tp"),
        P("ep", "tp", None),
    )
    return jax.shard_map(
        body,
        mesh=mesh,
        in_specs=placed,
        out_specs=(P("ep", "tp"), P("ep", "tp"), P("ep", "tp")),
        check_vma=False,
    )
```
